32 devices in a mesh: sp: 8 (over z, y), tp: 4 (over x, core).
Axes of the slice: x: 2, y: 2, z: 4, core: 2. Of those that a mesh axis runs over, the one named last changes fastest.
Arguments:
- queries: bfloat16 [6144, 2048], P('sp', 'tp'), may hold values from -11 to 11
- key_rows: bfloat16 [6144, 2048], P('sp', 'tp'), may hold values from -4.5 to 4.5
- value_rows: bfloat16 [6144, 2048], P('sp', 'tp'), may hold values from -6 to 6
- log_forget: float32 [6144, 32], P('sp', 'tp'), may hold values from -740.28 to 0, as said below
- stream_in: bfloat16 [6144, 2048], P('sp'), may hold values from -6 to 6
- out_weight: bfloat16 [2048, 2048], P('tp'), may hold values from -0.52734375 to 0.52734375
- mix_gain: float32 [2048], replicated, may hold values from 0.1 to 1.9
- mix_bias: float32 [2048], replicated, may hold values from -3 to 3
- gate_weight: bfloat16 [2048, 5632], P('sp', 'tp'), may hold values from -0.125 to 0.125
- up_weight: bfloat16 [2048, 5632], P('sp', 'tp'), may hold values from -0.125 to 0.125
- down_weight: bfloat16 [5632, 2048], P('tp', 'sp'), may hold values from -0.15917969 to 0.15917969
- ffn_gain: float32 [2048], replicated, may hold values from 0.1 to 1.9
- ffn_bias: float32 [2048], replicated, may hold values from -3 to 3
Outputs:
- layer_out: bfloat16 [6144, 2048], P(('sp', 'tp'))
The draws below stay inside these ranges and needn't reach their ends.
Inputs may be any that keep to these rules, and one draw needn't show every extreme that they name: `log_forget`: each column never rises along the positions.
All inputs are finite; a program needn't handle non-finite values.
Results may differ from the reference program's by a relative error of at most 0.015.
Values may be sent and summed in bfloat16 or wider, within the bound.
A program may use at most 128 MiB of HBM per device.

```python
import math
import jax
import jax.numpy as jnp
from jax import lax

D = 2048
HEAD_TOTAL = 32
FF = 5632
TOK_DEV = 768
SEQUENCE_LENGTH = 6144
N_SP = 8


def draw_queries(key, part):
    base_noise = jax.random.normal(jax.random.fold_in(key, 1), (SEQUENCE_LENGTH, D), jnp.float32)
    row_scale = jnp.exp(jax.random.uniform(jax.random.fold_in(key, 31), (SEQUENCE_LENGTH, 1), jnp.float32, -0.7, 1.6))
    base_noise = jnp.clip(base_noise * row_scale, -11.0, 11.0)
    return base_noise.astype(jnp.bfloat16)


def draw_key_rows(key, part):
    base_noise = jax.random.normal(jax.random.fold_in(key, 2), (SEQUENCE_LENGTH, D), jnp.float32)
    row_scale = jnp.exp(jax.random.uniform(jax.random.fold_in(key, 32), (SEQUENCE_LENGTH, 1), jnp.float32, -0.8, 0.8))
    base_noise = jnp.clip(base_noise * row_scale, -4.5, 4.5)
    return base_noise.astype(jnp.bfloat16)


def draw_log_forget(key, part):
    head_order = jax.random.permutation(jax.random.fold_in(key, 21), HEAD_TOTAL)
    sluggish_heads = head_order < HEAD_TOTAL // 2
    fast_rate = jnp.exp(jax.random.uniform(jax.random.fold_in(key, 22), (HEAD_TOTAL,), jnp.float32, math.log(1.0 / 100.0), math.log(1.0 / 30.0)))
    head_rate = jnp.where(sluggish_heads, 0.5 / SEQUENCE_LENGTH, fast_rate)
    block_count = SEQUENCE_LENGTH // TOK_DEV
    block_factor = jnp.exp(jax.random.uniform(jax.random.fold_in(key, 23), (block_count, HEAD_TOTAL), jnp.float32, math.log(0.5), math.log(2.0)))
    position_factor = jax.random.uniform(jax.random.fold_in(key, 24), (SEQUENCE_LENGTH, HEAD_TOTAL), jnp.float32, 0.25, 1.75)
    logarithm_increments = -head_rate[None, :] * jnp.repeat(block_factor, TOK_DEV, axis=0) * position_factor
    spike_locations = jax.random.randint(jax.random.fold_in(key, 25), (3, HEAD_TOTAL), 0, SEQUENCE_LENGTH)
    spike_lengths = jax.random.uniform(jax.random.fold_in(key, 26), (3, HEAD_TOTAL), jnp.float32, 0.22, 0.69)
    token_positions = jnp.arange(SEQUENCE_LENGTH, dtype=jnp.int32)
    for spike_index in range(3):
        spike_matches = (token_positions[:, None] == spike_locations[spike_index][None, :]) & sluggish_heads[None, :]
        logarithm_increments = logarithm_increments - jnp.where(spike_matches, spike_lengths[spike_index][None, :], 0.0)
    return jnp.cumsum(logarithm_increments, axis=0).astype(jnp.float32)


def levels(key, dims, cuts, low, largest):
    level, own = 1.0, jax.random.fold_in(key, 6)
    for axis_at, blocks in cuts:
        heights = jnp.exp(jax.random.uniform(jax.random.fold_in(own, axis_at), (blocks,), jnp.float32, low / len(cuts), largest / len(cuts)))
        level = level * jnp.repeat(heights, dims[axis_at] // blocks).reshape([-1 if axis == axis_at else 1 for axis in range(len(dims))])
    return level


def scatter_about(key, extent, width, most, split=(), kind=jnp.bfloat16):
    values = width * jax.random.normal(key, extent, jnp.float32)
    if split:
        values = values * levels(key, extent, split, -0.22, 0.18)
    return jnp.clip(values, -most, most).astype(kind)


def setup_inputs(seed: int = 0) -> dict:
    seeds = jax.random.split(jax.random.key(seed), 14)
    return {
        "queries": draw_queries(jax.random.fold_in(seeds[13], 71), 0),
        "key_rows": draw_key_rows(jax.random.fold_in(seeds[13], 71), 0),
        "value_rows": scatter_about(seeds[2], (SEQUENCE_LENGTH, D), 1.0, 6.0, ((0, 8), (1, 4))),
        "log_forget": draw_log_forget(jax.random.fold_in(seeds[13], 71), 0),
        "stream_in": scatter_about(seeds[4], (SEQUENCE_LENGTH, D), 1.0, 6.0, ((0, 8),)),
        "out_weight": scatter_about(seeds[5], (D, D), (4.0 * D ** -0.5), 0.52734375, ((0, 4),)),
        "mix_gain": jnp.clip(1.0 + 0.18 * jax.random.normal(seeds[6], (D,), jnp.float32), 0.1, 1.9),
        "mix_bias": scatter_about(seeds[7], (D,), 0.5, 3.0, (), jnp.float32),
        "gate_weight": scatter_about(seeds[8], (D, FF), D ** -0.5, 0.125, ((0, 8), (1, 4))),
        "up_weight": scatter_about(seeds[9], (D, FF), D ** -0.5, 0.125, ((0, 8), (1, 4))),
        "down_weight": scatter_about(seeds[10], (FF, D), (2.0 * FF ** -0.5), 0.15917969, ((0, 4), (1, 8))),
        "ffn_gain": jnp.clip(1.0 + 0.18 * jax.random.normal(seeds[11], (D,), jnp.float32), 0.1, 1.9),
        "ffn_bias": scatter_about(seeds[12], (D,), 0.5, 3.0, (), jnp.float32),
    }


ALPHA = 8.0 ** 0.25
EPSILON = 1e-05

def layer_norm(matrix, norm_gain, norm_shift):
    centred = matrix - lax.optimization_barrier(jnp.mean(matrix, axis=-1, keepdims=True))
    spread = lax.optimization_barrier(jnp.mean(centred * centred, axis=-1, keepdims=True))
    return centred * lax.rsqrt(spread + EPSILON) * norm_gain + norm_shift

def head_attention(query_head, key_head, value_head, gate_head):
    head_dim = query_head.shape[1]
    score_scale = head_dim ** (-0.5)
    key_pos = jnp.arange(SEQUENCE_LENGTH, dtype=jnp.int32)
    query_blocks = query_head.reshape(N_SP, TOK_DEV, head_dim)
    gate_blocks = gate_head.reshape(N_SP, TOK_DEV)

    def one_block(packed):
        query_block, gate_block, block_index = packed
        scores = jnp.dot(query_block, key_head.T, preferred_element_type=jnp.float32) * score_scale
        scores = scores + gate_block[:, None] - gate_head[None, :]
        query_pos = block_index * TOK_DEV + jnp.arange(TOK_DEV, dtype=jnp.int32)
        allowed = key_pos[None, :] <= query_pos[:, None]
        masked = jnp.where(allowed, scores, -1e+30)
        highest = lax.optimization_barrier(jnp.max(masked, axis=1, keepdims=True))
        exponent = jnp.where(allowed, jnp.exp(masked - highest), 0.0)
        totals = lax.optimization_barrier(jnp.sum(exponent, axis=1, keepdims=True))
        weighted = jnp.dot(exponent.astype(jnp.bfloat16), value_head, preferred_element_type=jnp.float32)
        return (weighted / totals).astype(jnp.bfloat16)
    return lax.map(one_block, (query_blocks, gate_blocks, jnp.arange(N_SP, dtype=jnp.int32)))

def reference(queries, key_rows, value_rows, log_forget, stream_in, out_weight, mix_gain, mix_bias, gate_weight, up_weight, down_weight, ffn_gain, ffn_bias):
    head_count = log_forget.shape[1]
    head_dim = queries.shape[1] // head_count

    def split_heads(matrix):
        return matrix.reshape(SEQUENCE_LENGTH, head_count, head_dim).transpose(1, 0, 2)

    def per_head(packed):
        return head_attention(packed[0], packed[1], packed[2], packed[3])
    attended = lax.map(per_head, (split_heads(queries), split_heads(key_rows), split_heads(value_rows), log_forget.T))
    attended = attended.reshape(head_count, SEQUENCE_LENGTH, head_dim).transpose(1, 0, 2).reshape(SEQUENCE_LENGTH, head_count * head_dim)
    mix_out = jnp.dot(attended, out_weight, preferred_element_type=jnp.float32).astype(jnp.bfloat16)
    mix_out = lax.optimization_barrier(mix_out).astype(jnp.float32)
    normed = layer_norm(ALPHA * stream_in.astype(jnp.float32) + mix_out, mix_gain, mix_bias).astype(jnp.bfloat16)
    gate_part = jnp.dot(normed, gate_weight, preferred_element_type=jnp.float32)
    up_part = jnp.dot(normed, up_weight, preferred_element_type=jnp.float32)
    hidden = (jax.nn.silu(gate_part) * up_part).astype(jnp.bfloat16)
    lowered = jnp.dot(hidden, down_weight, preferred_element_type=jnp.float32).astype(jnp.bfloat16)
    lowered = lax.optimization_barrier(lowered).astype(jnp.float32)
    result = layer_norm(ALPHA * normed.astype(jnp.float32) + lowered, ffn_gain, ffn_bias)
    return result.astype(jnp.bfloat16)
```

```python
import jax
import jax.numpy as jnp
from jax import lax
from jax.experimental import pallas as pl
from jax.experimental.pallas import tpu as pltpu
from jax.sharding import PartitionSpec as P


ALPHA = 8.0**0.25
EPSILON = 1e-05


def layer_norm(matrix, norm_gain, norm_shift):
    centred = matrix - jnp.mean(matrix, axis=-1, keepdims=True)
    spread = jnp.mean(centred * centred, axis=-1, keepdims=True)
    return centred * lax.rsqrt(spread + EPSILON) * norm_gain + norm_shift


def attend(queries, key_rows, value_rows, log_forget):
    length, row_width = queries.shape
    head_count = log_forget.shape[1]
    head_dim = row_width // head_count
    score_scale = head_dim ** (-0.5)
    first_pos = lax.axis_index("sp") * length
    last_pos = first_pos + length
    query_heads = queries.reshape(length, head_count, head_dim)
    query_gates = log_forget.T
    query_pos = first_pos + jnp.arange(length, dtype=jnp.int32)
    gates_all = lax.all_gather(log_forget, "sp", axis=0, tiled=True)
    initial = (
        jnp.full((head_count, length), -1e30, jnp.float32),
        jnp.zeros((head_count, length), jnp.float32),
        jnp.zeros((length, head_count, head_dim), jnp.float32),
    )
    running = initial
    key_piece = lax.all_gather(key_rows, "sp", axis=0, tiled=True)
    value_piece = lax.all_gather(value_rows, "sp", axis=0, tiled=True)
    piece_len = key_piece.shape[0]
    shards = piece_len // length
    group_size = max(
        [
            count_try
            for count_try in range(1, shards + 1)
            if shards % count_try == 0 and count_try * length <= max(length, 512)
        ]
    )
    block_len = group_size * length
    blocks = piece_len // block_len
    key_blocks = key_piece.reshape(blocks, block_len, head_count, head_dim)
    value_blocks = value_piece.reshape(blocks, block_len, head_count, head_dim)
    gate_blocks = gates_all.reshape(blocks, block_len, head_count)
    block_starts = block_len * jnp.arange(blocks, dtype=jnp.int32)

    def one_block(running_state, packed):
        key_block, value_block, gate_block, block_start = packed

        def compute(state_in):
            highest, totals, weighted = state_in
            scores = (
                jnp.einsum(
                    "qhd,khd->hqk", query_heads, key_block, preferred_element_type=jnp.float32
                )
                * score_scale
            )
            scores = scores + query_gates[:, :, None] - gate_block.T[:, None, :]
            key_pos = block_start + jnp.arange(block_len, dtype=jnp.int32)
            allowed = (key_pos[None, :] <= query_pos[:, None])[None]
            masked = jnp.where(allowed, scores, -1e30)
            new_high = jnp.maximum(highest, jnp.max(masked, axis=2))
            weights = jnp.where(allowed, jnp.exp(masked - new_high[:, :, None]), 0.0)
            factor = jnp.exp(highest - new_high)
            totals = totals * factor + jnp.sum(weights, axis=2)
            weighted = weighted * factor.T[:, :, None] + jnp.einsum(
                "hqk,khd->qhd",
                weights.astype(jnp.bfloat16),
                value_block,
                preferred_element_type=jnp.float32,
            )
            return (new_high, totals, weighted)

        def keep_state(state_in):
            return state_in

        return (lax.cond(block_start < last_pos, compute, keep_state, running_state), None)

    running, unused = lax.scan(
        one_block, running, (key_blocks, value_blocks, gate_blocks, block_starts)
    )
    highest, totals, weighted = running
    return (weighted / totals.T[:, :, None]).reshape(length, row_width).astype(jnp.bfloat16)


SUB = 256


def pack_pieces(queries, key_rows, value_rows, log_forget):
    length, row_width = queries.shape
    heads = log_forget.shape[1]
    head_dim = row_width // heads

    def turn(matrix):
        return matrix.T.reshape(heads, head_dim, length)

    gates = log_forget.T
    high = lax.reduce_precision(gates, 8, 7)
    middle = lax.reduce_precision(gates - high, 8, 7)
    low = gates - high - middle
    gate_rows = jnp.stack([high, middle, low], axis=1).astype(jnp.bfloat16)
    gate_rows = jnp.pad(gate_rows, ((0, 0), (0, 13), (0, 0)))
    return jnp.concatenate(
        [turn(key_rows), gate_rows, turn(queries), turn(value_rows)], axis=1
    )


def flash_piece(index, recv, kk, vaug, qaug, high_ref, acc_ref, head_dim):
    length = recv.shape[2]
    sub = SUB if length % SUB == 0 else length
    scale = head_dim**-0.5
    gate_rows = recv.shape[1] - 3 * head_dim
    query_at = head_dim + gate_rows
    value_at = query_at + head_dim
    kk[index] = recv[index, 0:128, :].T
    vaug[index, 0:head_dim, :] = recv[index, value_at : value_at + head_dim, :]
    row_index = lax.broadcasted_iota(jnp.int32, (gate_rows, length), 0)
    vaug[index, head_dim : head_dim + gate_rows, :] = jnp.where(row_index < 1, 1.0, 0.0).astype(
        jnp.bfloat16
    )
    block = recv[index, query_at : query_at + head_dim, :]
    qaug[0:head_dim, :] = (block.astype(jnp.float32) * scale).astype(jnp.bfloat16)
    qaug[head_dim : head_dim + gate_rows, :] = jnp.where(row_index < 3, -1.0, 0.0).astype(
        jnp.bfloat16
    )
    qaug[head_dim + gate_rows : 128, :] = jnp.zeros(
        (128 - head_dim - gate_rows, length), jnp.bfloat16
    )
    high_ref[...] = jnp.full_like(high_ref, -1e30)
    acc_ref[...] = jnp.zeros_like(acc_ref)

    def pair(piece, diagonal):
        for start in range(0, length, sub):
            width = min(length, start + sub) if diagonal else length
            scores = jnp.dot(
                kk[piece, 0:width, :],
                qaug[:, start : start + sub],
                preferred_element_type=jnp.float32,
            )
            if diagonal:
                key_pos = lax.broadcasted_iota(jnp.int32, (width, sub), 0)
                query_pos = start + lax.broadcasted_iota(jnp.int32, (width, sub), 1)
                scores = jnp.where(key_pos <= query_pos, scores, -1e30)
            old_high = high_ref[:, start : start + sub]
            new_high = jnp.maximum(old_high, jnp.max(scores, axis=0, keepdims=True))
            weights = jnp.exp(scores - new_high).astype(jnp.bfloat16)
            factor = jnp.exp(old_high - new_high)
            high_ref[:, start : start + sub] = new_high
            acc_ref[:, start : start + sub] = acc_ref[:, start : start + sub] * factor + jnp.dot(
                vaug[piece, :, 0:width], weights, preferred_element_type=jnp.float32
            )

    def earlier(piece, inner):
        pair(piece, False)
        return inner

    lax.fori_loop(0, index, earlier, 0)
    pair(index, True)
    return (acc_ref[0:head_dim, :] / acc_ref[head_dim : head_dim + 1, :]).astype(jnp.bfloat16)


def layer_kernel(
    packed,
    g_ref,
    u_ref,
    d_ref,
    ow_ref,
    st_ref,
    mg_ref,
    mb_ref,
    fg_ref,
    fb_ref,
    out_ref,
    recv,
    kk,
    vaug,
    qaug,
    high_ref,
    acc_ref,
    outp,
    att,
    attT,
    wt,
    wbuf,
    owv,
    stv,
    psend,
    precv,
    pown,
    xs,
    xr,
    nb,
    hid,
    dsend,
    drecv,
    dacc,
    rsb,
    r1,
    r2,
    local_sem,
    own_sem,
    a_send,
    a_recv,
    b_send,
    b_recv,
    y_send,
    y_recv,
    w_sem,
    z_send,
    z_recv,
    p_send,
    p_recv,
    x_send,
    x_recv,
    g_send,
    g_recv,
    d_send,
    d_recv,
    r_send,
    r_recv,
):
    n_sp = lax.axis_size("sp")
    slabs = n_sp // 2
    sp = lax.axis_index("sp")
    tp = lax.axis_index("tp")
    z, y = sp // 2, sp % 2
    x, c = tp // 2, tp % 2
    y_peer = (z * 2 + 1 - y, tp)
    x_peer = (sp, (1 - x) * 2 + c)
    c_peer = (sp, x * 2 + 1 - c)
    length = recv.shape[2]
    head_dim = outp.shape[1]
    rows = out_ref.shape[0]
    width = out_ref.shape[1]
    half = width // 2
    part = wt.shape[1] // 2
    cols = wt.shape[2]

    def remote(src, dst, send, receive, device):
        return pltpu.make_async_remote_copy(
            src_ref=src,
            dst_ref=dst,
            send_sem=send,
            recv_sem=receive,
            device_id=device,
            device_id_type=pl.DeviceIdType.MESH,
        )

    def piece_copy(other):
        return remote(
            packed.at[other], recv.at[sp], a_send.at[other], a_recv.at[sp], (other, tp)
        )

    def piece_wait(source):
        remote(
            packed.at[source], recv.at[source], a_send.at[source], a_recv.at[source], (source, tp)
        ).wait_recv()

    own_piece = pltpu.make_async_copy(packed.at[sp], recv.at[sp], own_sem.at[0])
    own_piece.start()

    def send_piece(step, carry):
        piece_copy((sp + step) % n_sp).start()
        return carry

    lax.fori_loop(1, n_sp, send_piece, 0)
    load_ow = pltpu.make_async_copy(ow_ref, owv, local_sem.at[0])
    load_st = pltpu.make_async_copy(st_ref.at[pl.ds(tp * rows, rows), :], stv, local_sem.at[1])
    load_ow.start()
    load_st.start()

    wt[0] = g_ref[...].T
    wt[1] = u_ref[...].T

    def chunk(matrix, owner, count):
        return wbuf.at[matrix, :, pl.ds(pl.multiple_of(owner * cols, cols), count * cols)]

    def weight_rows(matrix, which):
        taken = pl.ds(which * part, part)
        return d_ref.at[taken, :] if matrix == 2 else wt.at[matrix, taken, :]

    def keep_copy(matrix):
        return pltpu.make_async_copy(
            weight_rows(matrix, y), chunk(matrix, sp, 1), w_sem.at[matrix]
        )

    def cross_copy(matrix):
        return remote(
            weight_rows(matrix, 1 - y),
            chunk(matrix, sp, 1),
            y_send.at[matrix],
            y_recv.at[matrix],
            y_peer,
        )

    def cross_wait(matrix):
        peer_chunk = chunk(matrix, z * 2 + 1 - y, 1)
        remote(
            peer_chunk, peer_chunk, y_send.at[matrix], y_recv.at[matrix], y_peer
        ).wait_recv()

    for matrix in range(3):
        keep_copy(matrix).start()
        cross_copy(matrix).start()

    def z_copy(way, stage, matrix):
        if way == 0:
            given, allowed = z - stage, (z >= stage) & (z + 1 < slabs)
            device = (sp + 2, tp)
        else:
            given, allowed = z + stage, (z + stage < slabs) & (z >= 1)
            device = (sp - 2, tp)
        block = chunk(matrix, given * 2, 2)
        copy = remote(
            block, block, z_send.at[way, stage, matrix], z_recv.at[way, stage, matrix], device
        )
        return copy, allowed

    def z_start(stage, matrix):
        for way in range(2):
            copy, allowed = z_copy(way, stage, matrix)

            @pl.when(allowed)
            def _():
                copy.start()

    def z_wait(stage, matrix):
        for way in range(2):
            if way == 0:
                taken, allowed = z - 1 - stage, z >= 1 + stage
                device = (sp - 2, tp)
            else:
                taken, allowed = z + 1 + stage, z + 1 + stage < slabs
                device = (sp + 2, tp)

            @pl.when(allowed)
            def _():
                block = chunk(matrix, taken * 2, 2)
                remote(
                    block,
                    block,
                    z_send.at[way, stage, matrix],
                    z_recv.at[way, stage, matrix],
                    device,
                ).wait_recv()

    def z_first(matrix):
        keep_copy(matrix).wait()
        cross_wait(matrix)
        z_start(0, matrix)

    def z_relay(stage, matrix):
        z_wait(stage, matrix)
        if stage + 1 < slabs - 1:
            z_start(stage + 1, matrix)

    def back_copy(piece):
        return remote(
            outp.at[piece],
            att.at[pl.ds(sp * head_dim, head_dim), :],
            b_send.at[piece],
            b_recv.at[sp],
            (piece, tp),
        )

    def back_wait(source):
        remote(
            outp.at[source],
            att.at[pl.ds(source * head_dim, head_dim), :],
            b_send.at[source],
            b_recv.at[source],
            (source, tp),
        ).wait_recv()

    own_back = pltpu.make_async_copy(
        outp.at[sp], att.at[pl.ds(sp * head_dim, head_dim), :], own_sem.at[1]
    )

    def one_piece(index, carry):
        @pl.when(index == sp)
        def _():
            own_piece.wait()

        @pl.when(index != sp)
        def _():
            piece_wait(index)

        outp[index] = flash_piece(index, recv, kk, vaug, qaug, high_ref, acc_ref, head_dim)

        @pl.when(index == sp)
        def _():
            own_back.start()

        @pl.when(index != sp)
        def _():
            back_copy(index).start()

        for at, stage, matrix in RELAYS:

            @pl.when(index == at)
            def _():
                if stage < 0:
                    z_first(matrix)
                else:
                    z_relay(stage, matrix)

        return carry

    lax.fori_loop(0, n_sp, one_piece, 0)

    own_back.wait()

    def wait_back(step, carry):
        back_wait((sp + step) % n_sp)
        return carry

    lax.fori_loop(1, n_sp, wait_back, 0)
    load_ow.wait()
    load_st.wait()
    attT[...] = att[...].T

    def mix_block(owner):
        return jnp.dot(
            attT[pl.ds(owner * rows, rows), :], owv[...], preferred_element_type=jnp.float32
        )

    def pair_copy(slot):
        return remote(psend.at[slot], precv.at[slot], p_send.at[slot], p_recv.at[slot], c_peer)

    def mix_away(slot, carry):
        psend[slot] = mix_block(((x + 1 + slot) % 2) * 2 + 1 - c).astype(jnp.bfloat16)
        pair_copy(slot).start()
        return carry

    lax.fori_loop(0, 2, mix_away, 0)

    def mix_own(slot, carry):
        pown[slot] = mix_block(((x + 1 + slot) % 2) * 2 + c)
        return carry

    lax.fori_loop(0, 2, mix_own, 0)
    pair_copy(0).wait_recv()
    xs[...] = (pown[0] + precv[0].astype(jnp.float32)).astype(jnp.bfloat16)
    across = remote(xs, xr, x_send.at[0], x_recv.at[0], x_peer)
    across.start()
    for stage, matrix in RELAYS_ACROSS:
        if stage < 0:
            z_first(matrix)
        else:
            z_relay(stage, matrix)
    pair_copy(1).wait_recv()
    across.wait_recv()

    def place(by, bx, bc):
        return ((y + by) % 2) * 4 + ((x + bx) % 2) * 2 + (c + bc) % 2

    own = place(0, 0, 0)
    tile = 16

    def norm(matrix, gain, shift):
        centred = matrix - jnp.mean(matrix, axis=-1, keepdims=True)
        spread = jnp.mean(centred * centred, axis=-1, keepdims=True)
        return (centred * lax.rsqrt(spread + EPSILON) * gain + shift).astype(jnp.bfloat16)

    def mix_norm(step, carry):
        at = pl.ds(pl.multiple_of(step * tile, tile), tile)
        summed = pown[1, at, :] + precv[1, at, :].astype(jnp.float32)
        summed = (summed + xr[at, :].astype(jnp.float32)).astype(jnp.bfloat16)
        nb[own, at, :] = norm(
            ALPHA * stv[at, :].astype(jnp.float32) + summed.astype(jnp.float32),
            mg_ref[...],
            mb_ref[...],
        )
        return carry

    lax.fori_loop(0, rows // tile, mix_norm, 0)

    top = pl.ds(0, rows // 2)
    bottom = pl.ds(rows // 2, rows // 2)

    def block_copy(sem, block, device):
        return remote(nb.at[block], nb.at[block], g_send.at[sem], g_recv.at[sem], device)

    def half_copy(sem, block, taken, device):
        view = nb.at[block, taken, :]
        return remote(view, view, g_send.at[sem], g_recv.at[sem], device)

    gathers = [
        block_copy(0, own, c_peer),
        block_copy(1, own, x_peer),
        block_copy(2, own, y_peer),
        half_copy(3, place(0, 1, 0), top, y_peer),
        half_copy(4, place(1, 0, 0), bottom, x_peer),
        block_copy(5, place(0, 1, 0), c_peer),
        block_copy(6, place(1, 0, 0), c_peer),
        block_copy(7, place(1, 1, 0), c_peer),
    ]
    arrivals = [
        block_copy(0, place(0, 0, 1), c_peer),
        block_copy(1, place(0, 1, 0), x_peer),
        block_copy(2, place(1, 0, 0), y_peer),
        half_copy(3, place(1, 1, 0), top, y_peer),
        half_copy(4, place(1, 1, 0), bottom, x_peer),
        block_copy(5, place(0, 1, 1), c_peer),
        block_copy(6, place(1, 0, 1), c_peer),
        block_copy(7, place(1, 1, 1), c_peer),
    ]
    gathers[1].start()
    gathers[2].start()
    gathers[0].start()
    for stage, matrix in RELAYS_GATHER:
        if stage < 0:
            z_first(matrix)
        else:
            z_relay(stage, matrix)

    def up_block(step):
        by, bx = step // 2, step % 2
        first = place(by, bx, 0) // 2
        block = nb[pl.ds(first * 2, 2)].reshape(2 * rows, width)
        contract = (((1,), (1,)), ((), ()))
        gate = lax.dot_general(block, wbuf[0], contract, preferred_element_type=jnp.float32)
        up = lax.dot_general(block, wbuf[1], contract, preferred_element_type=jnp.float32)
        hid[step] = (gate / (1.0 + jnp.exp(-gate)) * up).astype(jnp.bfloat16)

    def forward(step, carry):
        @pl.when(step == 0)
        def _():
            arrivals[0].wait_recv()

        @pl.when(step == 1)
        def _():
            arrivals[1].wait_recv()
            gathers[3].start()
            gathers[5].start()
            arrivals[2].wait_recv()
            gathers[4].start()
            gathers[6].start()
            arrivals[5].wait_recv()

        @pl.when(step == 2)
        def _():
            arrivals[6].wait_recv()

        @pl.when(step == 3)
        def _():
            arrivals[3].wait_recv()
            arrivals[4].wait_recv()
            gathers[7].start()
            arrivals[7].wait_recv()

        up_block(step)
        return carry

    lax.fori_loop(0, 4, forward, 0)
    for stage, matrix in RELAYS_DOWN:
        z_relay(stage, matrix)

    def core_copy(step):
        return remote(dsend.at[step], drecv.at[step], d_send.at[step], d_recv.at[step], c_peer)

    left = pl.ds(0, half)
    right = pl.ds(half, half)
    outs = [
        remote(rsb.at[0, :, left], r1.at[0], r_send.at[0], r_recv.at[0], x_peer),
        remote(rsb.at[1, :, left], r1.at[1], r_send.at[1], r_recv.at[1], x_peer),
        remote(rsb.at[0, :, right], r1.at[2], r_send.at[2], r_recv.at[2], y_peer),
        remote(rsb.at[2, :, right], r1.at[3], r_send.at[3], r_recv.at[3], y_peer),
        remote(rsb.at[2, :, left], r2.at[0], r_send.at[4], r_recv.at[4], y_peer),
        remote(rsb.at[1, :, right], r2.at[1], r_send.at[5], r_recv.at[5], x_peer),
    ]

    def core_sum(step):
        core_copy(step).wait_recv()
        dacc[step] = dacc[step] + drecv[step].astype(jnp.float32)

    def down_step(step, carry):
        slot = 3 - step
        slot = (slot // 2) + 2 * (slot % 2)
        given = hid[slot, pl.ds((1 - c) * rows, rows), :]
        dsend[step] = jnp.dot(given, wbuf[2], preferred_element_type=jnp.float32).astype(
            jnp.bfloat16
        )
        core_copy(step).start()
        kept = hid[slot, pl.ds(c * rows, rows), :]
        dacc[step] = jnp.dot(kept, wbuf[2], preferred_element_type=jnp.float32)
        core_sum(step)

        @pl.when(step == 0)
        def _():
            rsb[0] = dacc[0].astype(jnp.bfloat16)
            outs[0].start()
            outs[2].start()

        @pl.when(step == 1)
        def _():
            rsb[1, :, left] = dacc[1, :, left].astype(jnp.bfloat16)
            outs[1].start()

        @pl.when(step == 2)
        def _():
            rsb[2, :, right] = dacc[2, :, right].astype(jnp.bfloat16)
            outs[3].start()

        return carry

    lax.fori_loop(0, 4, down_step, 0)
    outs[0].wait_recv()
    rsb[2, :, left] = (dacc[2, :, left] + r1[0].astype(jnp.float32)).astype(jnp.bfloat16)
    outs[4].start()
    outs[2].wait_recv()
    rsb[1, :, right] = (dacc[1, :, right] + r1[2].astype(jnp.float32)).astype(jnp.bfloat16)
    outs[5].start()
    outs[1].wait_recv()
    outs[3].wait_recv()
    outs[4].wait_recv()
    outs[5].wait_recv()

    def last_norm(step, carry):
        at = pl.ds(pl.multiple_of(step * tile, tile), tile)
        low = dacc[3, at, left] + r1[1, at, :].astype(jnp.float32) + r2[0, at, :].astype(jnp.float32)
        high = (
            dacc[3, at, right] + r1[3, at, :].astype(jnp.float32) + r2[1, at, :].astype(jnp.float32)
        )
        lowered = jnp.concatenate([low, high], axis=1).astype(jnp.bfloat16).astype(jnp.float32)
        out_ref[at, :] = norm(
            ALPHA * nb[own, at, :].astype(jnp.float32) + lowered, fg_ref[...], fb_ref[...]
        )
        return carry

    lax.fori_loop(0, rows // tile, last_norm, 0)

    def sent_pieces(step, carry):
        piece_copy((sp + step) % n_sp).wait_send()
        back_copy((sp + step) % n_sp).wait_send()
        return carry

    lax.fori_loop(1, n_sp, sent_pieces, 0)
    for matrix in range(3):
        cross_copy(matrix).wait_send()
        for way in range(2):
            for stage in range(slabs - 1):
                copy, allowed = z_copy(way, stage, matrix)

                @pl.when(allowed)
                def _():
                    copy.wait_send()

    pair_copy(0).wait_send()
    pair_copy(1).wait_send()
    across.wait_send()
    for copy in gathers:
        copy.wait_send()
    for step in range(4):
        core_copy(step).wait_send()
    for copy in outs:
        copy.wait_send()


RELAYS = ((1, -1, 0), (2, -1, 1), (5, 0, 0), (6, 0, 1), (7, 1, 0))
RELAYS_ACROSS = ((1, 1), (-1, 2))
RELAYS_GATHER = ((0, 2), (2, 0), (2, 1))
RELAYS_DOWN = ((1, 2), (2, 2))


def whole_layer(
    queries,
    key_rows,
    value_rows,
    log_forget,
    stream_in,
    out_weight,
    mix_gain,
    mix_bias,
    gate_weight,
    up_weight,
    down_weight,
    ffn_gain,
    ffn_bias,
):
    length, row_width = queries.shape
    heads = log_forget.shape[1]
    head_dim = row_width // heads
    pieces = lax.axis_size("sp")
    slabs = pieces // 2
    rows = length // lax.axis_size("tp")
    width = stream_in.shape[1]
    cols, hidden = gate_weight.shape
    part = hidden // 2
    packed = pack_pieces(queries, key_rows, value_rows, log_forget)
    high_rows = packed.shape[1] - 2 * head_dim
    bf16, f32 = jnp.bfloat16, jnp.float32
    vmem, dma = pltpu.VMEM, pltpu.SemaphoreType.DMA
    scratch = [
        vmem((pieces,) + packed.shape[1:], bf16),
        vmem((pieces, length, 128), bf16),
        vmem((pieces, high_rows, length), bf16),
        vmem((128, length), bf16),
        vmem((1, length), f32),
        vmem((high_rows, length), f32),
        vmem((pieces, head_dim, length), bf16),
        vmem((row_width, length), bf16),
        vmem((length, row_width), bf16),
        vmem((2, hidden, cols), bf16),
        vmem((3, part, width), bf16),
        vmem((row_width, width), bf16),
        vmem((rows, width), bf16),
        vmem((2, rows, width), bf16),
        vmem((2, rows, width), bf16),
        vmem((2, rows, width), f32),
        vmem((rows, width), bf16),
        vmem((rows, width), bf16),
        vmem((8, rows, width), bf16),
        vmem((4, 2 * rows, part), bf16),
        vmem((4, rows, width), bf16),
        vmem((4, rows, width), bf16),
        vmem((4, rows, width), f32),
        vmem((3, rows, width), bf16),
        vmem((4, rows, width // 2), bf16),
        vmem((2, rows, width // 2), bf16),
        dma((2,)),
        dma((2,)),
        dma((pieces,)),
        dma((pieces,)),
        dma((pieces,)),
        dma((pieces,)),
        dma((3,)),
        dma((3,)),
        dma((3,)),
        dma((2, slabs - 1, 3)),
        dma((2, slabs - 1, 3)),
        dma((2,)),
        dma((2,)),
        dma((1,)),
        dma((1,)),
        dma((8,)),
        dma((8,)),
        dma((4,)),
        dma((4,)),
        dma((6,)),
        dma((6,)),
    ]
    in_vmem = pl.BlockSpec(memory_space=pltpu.VMEM)
    anywhere = pl.BlockSpec(memory_space=pl.ANY)
    return pl.pallas_call(
        layer_kernel,
        out_shape=jax.ShapeDtypeStruct((rows, width), bf16),
        in_specs=[anywhere, in_vmem, in_vmem, anywhere, anywhere, anywhere] + [in_vmem] * 4,
        out_specs=in_vmem,
        scratch_shapes=scratch,
        compiler_params=pltpu.CompilerParams(
            vmem_limit_bytes=67043328, has_side_effects=True
        ),
    )(
        packed,
        gate_weight,
        up_weight,
        down_weight,
        out_weight,
        stream_in,
        mix_gain[None, :],
        mix_bias[None, :],
        ffn_gain[None, :],
        ffn_bias[None, :],
    )


def swap_cores(block):
    count = lax.axis_size("tp")
    return lax.ppermute(block, "tp", [(i, i ^ 1) for i in range(count)])


def swap_across(block):
    count = lax.axis_size("tp")
    return lax.ppermute(block, "tp", [(i, i ^ 2) for i in range(count)])


def body(
    queries,
    key_rows,
    value_rows,
    log_forget,
    stream_in,
    out_weight,
    mix_gain,
    mix_bias,
    gate_weight,
    up_weight,
    down_weight,
    ffn_gain,
    ffn_bias,
):
    length = queries.shape[0]
    heads = log_forget.shape[1]
    head_dim = queries.shape[1] // heads
    pieces, group = lax.axis_size("sp"), lax.axis_size("tp")
    by_head = heads == pieces and head_dim + 16 <= 128 and head_dim % 16 == 0
    if by_head and pieces == 8 and group == 4:
        return whole_layer(
            queries,
            key_rows,
            value_rows,
            log_forget,
            stream_in,
            out_weight,
            mix_gain,
            mix_bias,
            gate_weight,
            up_weight,
            down_weight,
            ffn_gain,
            ffn_bias,
        )
    gate_full = lax.all_gather(gate_weight, "sp", axis=0, tiled=True)
    up_full = lax.all_gather(up_weight, "sp", axis=0, tiled=True)
    down_full = lax.all_gather(down_weight, "sp", axis=1, tiled=True)
    turned = attend(queries, key_rows, value_rows, log_forget).T
    own_rows = length // lax.axis_size("tp")
    offset = lax.axis_index("tp") * own_rows
    two_level = lax.axis_size("tp") == 4
    partial_mix = lax.dot_general(
        turned, out_weight, (((0,), (0,)), ((), ())), preferred_element_type=jnp.float32
    ).astype(jnp.bfloat16)
    if two_level:
        core = lax.axis_index("tp") % 2
        across = lax.axis_index("tp") // 2
        split = partial_mix.reshape(2, 2, own_rows, -1)
        mine = lax.dynamic_index_in_dim(split, core, 1, keepdims=False)
        other = lax.dynamic_index_in_dim(split, 1 - core, 1, keepdims=False)
        both = mine.astype(jnp.float32) + swap_cores(other).astype(jnp.float32)
        own = lax.dynamic_index_in_dim(both, across, 0, keepdims=False)
        away = lax.dynamic_index_in_dim(both, 1 - across, 0, keepdims=False)
        summed = (own + swap_across(away.astype(jnp.bfloat16)).astype(jnp.float32)).astype(
            jnp.bfloat16
        )
    else:
        summed = lax.psum_scatter(partial_mix, "tp", scatter_dimension=0, tiled=True)
    mix_out = lax.optimization_barrier(summed).astype(jnp.float32)
    stream_own = lax.dynamic_slice_in_dim(stream_in, offset, own_rows, 0)
    normed = layer_norm(
        ALPHA * stream_own.astype(jnp.float32) + mix_out, mix_gain, mix_bias
    ).astype(jnp.bfloat16)
    if two_level:
        pair = jnp.concatenate([normed, swap_across(normed)], axis=0)
        gathered = jnp.concatenate([pair, swap_cores(pair)], axis=0)
    else:
        gathered = lax.all_gather(normed, "tp", axis=0, tiled=True)
    gate_part = jnp.dot(gathered, gate_full, preferred_element_type=jnp.float32)
    up_part = jnp.dot(gathered, up_full, preferred_element_type=jnp.float32)
    hidden = (jax.nn.silu(gate_part) * up_part).astype(jnp.bfloat16)
    if two_level:
        columns = []
        half = down_full.shape[1] // 2
        for start in (0, half):
            terms = jnp.dot(
                hidden, down_full[:, start : start + half], preferred_element_type=jnp.float32
            ).astype(jnp.bfloat16)
            both = terms[: 2 * own_rows].astype(jnp.float32) + swap_cores(
                terms[2 * own_rows :]
            ).astype(jnp.float32)
            columns.append(
                both[:own_rows]
                + swap_across(both[own_rows:].astype(jnp.bfloat16)).astype(jnp.float32)
            )
        lowered = jnp.concatenate(columns, axis=1)
    else:
        partial_terms = jnp.dot(hidden, down_full, preferred_element_type=jnp.float32)
        lowered = lax.psum_scatter(
            partial_terms.astype(jnp.bfloat16), "tp", scatter_dimension=0, tiled=True
        ).astype(jnp.float32)
    lowered = lax.optimization_barrier(lowered.astype(jnp.bfloat16)).astype(jnp.float32)
    result = layer_norm(ALPHA * normed.astype(jnp.float32) + lowered, ffn_gain, ffn_bias)
    return result.astype(jnp.bfloat16)


def solution(mesh):
    placed = (
        P("sp", "tp"),
        P("sp", "tp"),
        P("sp", "tp"),
        P("sp", "tp"),
        P("sp", None),
        P("tp", None),
        P(),
        P(),
        P("sp", "tp"),
        P("sp", "tp"),
        P("tp", "sp"),
        P(),
        P(),
    )
    return jax.shard_map(
        body, mesh=mesh, in_specs=placed, out_specs=P(("sp", "tp"), None), check_vma=False
    )
```

```python
import jax
import jax.numpy as jnp
from jax import lax
from jax.experimental import pallas as pl
from jax.experimental.pallas import tpu as pltpu
from jax.sharding import PartitionSpec as P


ALPHA = 8.0**0.25
EPSILON = 1e-05


def layer_norm(matrix, norm_gain, norm_shift):
    centred = matrix - jnp.mean(matrix, axis=-1, keepdims=True)
    spread = jnp.mean(centred * centred, axis=-1, keepdims=True)
    return centred * lax.rsqrt(spread + EPSILON) * norm_gain + norm_shift


def attend(queries, key_rows, value_rows, log_forget):
    length, row_width = queries.shape
    head_count = log_forget.shape[1]
    head_dim = row_width // head_count
    score_scale = head_dim ** (-0.5)
    first_pos = lax.axis_index("sp") * length
    last_pos = first_pos + length
    query_heads = queries.reshape(length, head_count, head_dim)
    query_gates = log_forget.T
    query_pos = first_pos + jnp.arange(length, dtype=jnp.int32)
    gates_all = lax.all_gather(log_forget, "sp", axis=0, tiled=True)
    initial = (
        jnp.full((head_count, length), -1e30, jnp.float32),
        jnp.zeros((head_count, length), jnp.float32),
        jnp.zeros((length, head_count, head_dim), jnp.float32),
    )
    running = initial
    key_piece = lax.all_gather(key_rows, "sp", axis=0, tiled=True)
    value_piece = lax.all_gather(value_rows, "sp", axis=0, tiled=True)
    piece_len = key_piece.shape[0]
    shards = piece_len // length
    group_size = max(
        [
            count_try
            for count_try in range(1, shards + 1)
            if shards % count_try == 0 and count_try * length <= max(length, 512)
        ]
    )
    block_len = group_size * length
    blocks = piece_len // block_len
    key_blocks = key_piece.reshape(blocks, block_len, head_count, head_dim)
    value_blocks = value_piece.reshape(blocks, block_len, head_count, head_dim)
    gate_blocks = gates_all.reshape(blocks, block_len, head_count)
    block_starts = block_len * jnp.arange(blocks, dtype=jnp.int32)

    def one_block(running_state, packed):
        key_block, value_block, gate_block, block_start = packed

        def compute(state_in):
            highest, totals, weighted = state_in
            scores = (
                jnp.einsum(
                    "qhd,khd->hqk", query_heads, key_block, preferred_element_type=jnp.float32
                )
                * score_scale
            )
            scores = scores + query_gates[:, :, None] - gate_block.T[:, None, :]
            key_pos = block_start + jnp.arange(block_len, dtype=jnp.int32)
            allowed = (key_pos[None, :] <= query_pos[:, None])[None]
            masked = jnp.where(allowed, scores, -1e30)
            new_high = jnp.maximum(highest, jnp.max(masked, axis=2))
            weights = jnp.where(allowed, jnp.exp(masked - new_high[:, :, None]), 0.0)
            factor = jnp.exp(highest - new_high)
            totals = totals * factor + jnp.sum(weights, axis=2)
            weighted = weighted * factor.T[:, :, None] + jnp.einsum(
                "hqk,khd->qhd",
                weights.astype(jnp.bfloat16),
                value_block,
                preferred_element_type=jnp.float32,
            )
            return (new_high, totals, weighted)

        def keep_state(state_in):
            return state_in

        return (lax.cond(block_start < last_pos, compute, keep_state, running_state), None)

    running, unused = lax.scan(
        one_block, running, (key_blocks, value_blocks, gate_blocks, block_starts)
    )
    highest, totals, weighted = running
    return (weighted / totals.T[:, :, None]).reshape(length, row_width).astype(jnp.bfloat16)


SUB = 256


def pack_pieces(queries, key_rows, value_rows, log_forget):
    length, row_width = queries.shape
    heads = log_forget.shape[1]
    head_dim = row_width // heads

    def turn(matrix):
        return matrix.T.reshape(heads, head_dim, length)

    gates = log_forget.T
    high = lax.reduce_precision(gates, 8, 7)
    middle = lax.reduce_precision(gates - high, 8, 7)
    low = gates - high - middle
    gate_rows = jnp.stack([high, middle, low], axis=1).astype(jnp.bfloat16)
    gate_rows = jnp.pad(gate_rows, ((0, 0), (0, 13), (0, 0)))
    return jnp.concatenate(
        [turn(key_rows), gate_rows, turn(queries), turn(value_rows)], axis=1
    )


def flash_piece(index, recv, kk, vaug, qaug, high_ref, acc_ref, head_dim):
    length = recv.shape[2]
    sub = SUB if length % SUB == 0 else length
    scale = head_dim**-0.5
    gate_rows = recv.shape[1] - 3 * head_dim
    query_at = head_dim + gate_rows
    value_at = query_at + head_dim
    kk[index] = recv[index, 0:128, :].T
    vaug[index, 0:head_dim, :] = recv[index, value_at : value_at + head_dim, :]
    row_index = lax.broadcasted_iota(jnp.int32, (gate_rows, length), 0)
    vaug[index, head_dim : head_dim + gate_rows, :] = jnp.where(row_index < 1, 1.0, 0.0).astype(
        jnp.bfloat16
    )
    block = recv[index, query_at : query_at + head_dim, :]
    qaug[0:head_dim, :] = (block.astype(jnp.float32) * scale).astype(jnp.bfloat16)
    qaug[head_dim : head_dim + gate_rows, :] = jnp.where(row_index < 3, -1.0, 0.0).astype(
        jnp.bfloat16
    )
    qaug[head_dim + gate_rows : 128, :] = jnp.zeros(
        (128 - head_dim - gate_rows, length), jnp.bfloat16
    )
    high_ref[...] = jnp.full_like(high_ref, -1e30)
    acc_ref[...] = jnp.zeros_like(acc_ref)

    def pair(piece, diagonal):
        starts = range(0, length, sub)
        spans = [slice(start, start + sub) for start in starts]
        widths = [start + sub if diagonal else length for start in starts]
        all_scores = [
            jnp.dot(kk[piece, 0:width, :], qaug[:, span], preferred_element_type=jnp.float32)
            for span, width in zip(spans, widths)
        ]
        if diagonal:
            key_pos = lax.broadcasted_iota(jnp.int32, (sub, sub), 0)
            allowed = key_pos <= lax.broadcasted_iota(jnp.int32, (sub, sub), 1)
            cut = [jnp.where(allowed, scores[-sub:], -1e30) for scores in all_scores]
            all_scores = cut[:1] + [
                jnp.concatenate([scores[:-sub], last], axis=0)
                for scores, last in zip(all_scores[1:], cut[1:])
            ]
        for scores, span, width in zip(all_scores, spans, widths):
            old_high = high_ref[:, span]
            new_high = jnp.maximum(old_high, jnp.max(scores, axis=0, keepdims=True))
            weights = jnp.exp(scores - new_high).astype(jnp.bfloat16)
            factor = jnp.exp(old_high - new_high)
            high_ref[:, span] = new_high
            acc_ref[:, span] = acc_ref[:, span] * factor + jnp.dot(
                vaug[piece, :, 0:width], weights, preferred_element_type=jnp.float32
            )

    def earlier(piece, inner):
        pair(piece, False)
        return inner

    lax.fori_loop(0, index, earlier, 0)
    pair(index, True)
    return (acc_ref[0:head_dim, :] / acc_ref[head_dim : head_dim + 1, :]).astype(jnp.bfloat16)


def layer_kernel(
    packed,
    g_ref,
    u_ref,
    d_ref,
    ow_ref,
    st_ref,
    mg_ref,
    mb_ref,
    fg_ref,
    fb_ref,
    out_ref,
    recv,
    kk,
    vaug,
    qaug,
    high_ref,
    acc_ref,
    outp,
    att,
    attT,
    wt,
    wbuf,
    owv,
    stv,
    psend,
    precv,
    pown,
    xs,
    xr,
    nb,
    hid,
    dsend,
    drecv,
    dacc,
    rsb,
    r1,
    local_sem,
    own_sem,
    a_send,
    a_recv,
    b_send,
    b_recv,
    y_send,
    y_recv,
    w_sem,
    z_send,
    z_recv,
    p_send,
    p_recv,
    x_send,
    x_recv,
    g_send,
    g_recv,
    d_send,
    d_recv,
    r_send,
    r_recv,
):
    n_sp = lax.axis_size("sp")
    sp = lax.axis_index("sp")
    tp = lax.axis_index("tp")
    z, y = sp // 2, sp % 2
    x, c = tp // 2, tp % 2
    slabs = n_sp // 2
    y_peer = (z * 2 + 1 - y, tp)
    x_peer = (sp, (1 - x) * 2 + c)
    c_peer = (sp, x * 2 + 1 - c)
    length = recv.shape[2]
    head_dim = outp.shape[1]
    rows = out_ref.shape[0]
    width = out_ref.shape[1]
    part = wt.shape[1] // 2
    cols = wt.shape[2]

    def remote(src, dst, send, receive, device):
        return pltpu.make_async_remote_copy(
            src_ref=src,
            dst_ref=dst,
            send_sem=send,
            recv_sem=receive,
            device_id=device,
            device_id_type=pl.DeviceIdType.MESH,
        )

    barrier = pltpu.get_barrier_semaphore()

    def greet(step, carry):
        pl.semaphore_signal(
            barrier,
            inc=1,
            device_id=((sp + step) % n_sp, tp),
            device_id_type=pl.DeviceIdType.MESH,
        )
        return carry

    lax.fori_loop(1, n_sp, greet, 0)
    for device in (x_peer, c_peer):
        pl.semaphore_signal(
            barrier, inc=1, device_id=device, device_id_type=pl.DeviceIdType.MESH
        )
    wt[0] = g_ref[...].T
    wt[1] = u_ref[...].T
    pl.semaphore_wait(barrier, n_sp + 1)

    def piece_copy(other):
        return remote(
            packed.at[other], recv.at[sp], a_send.at[other], a_recv.at[sp], (other, tp)
        )

    def piece_wait(source):
        remote(
            packed.at[source], recv.at[source], a_send.at[source], a_recv.at[source], (source, tp)
        ).wait_recv()

    own_piece = pltpu.make_async_copy(packed.at[sp], recv.at[sp], own_sem.at[0])
    own_piece.start()

    def send_piece(step, carry):
        piece_copy((sp + n_sp - step) % n_sp).start()
        return carry

    lax.fori_loop(1, n_sp, send_piece, 0)
    load_ow = pltpu.make_async_copy(ow_ref, owv, local_sem.at[0])
    load_st = pltpu.make_async_copy(st_ref.at[pl.ds(tp * rows, rows), :], stv, local_sem.at[1])
    load_ow.start()
    load_st.start()

    inner = (z > 0) & (z + 1 < slabs)

    def chunk(matrix, owner, count):
        return wbuf.at[matrix, :, pl.ds(pl.multiple_of(owner * cols, cols), count * cols)]

    def weight_rows(matrix, which):
        taken = pl.ds(which * part, part)
        return d_ref.at[taken, :] if matrix == 2 else wt.at[matrix, taken, :]

    def keep_copy(matrix):
        return pltpu.make_async_copy(
            weight_rows(matrix, y), chunk(matrix, sp, 1), w_sem.at[matrix]
        )

    def cross_copy(matrix):
        return remote(
            weight_rows(matrix, 1 - y),
            chunk(matrix, sp, 1),
            y_send.at[matrix],
            y_recv.at[matrix],
            y_peer,
        )

    def cross_wait(matrix):
        block = chunk(matrix, z * 2 + 1 - y, 1)
        remote(block, block, y_send.at[matrix], y_recv.at[matrix], y_peer).wait_recv()

    for matrix in range(3):
        cross_copy(matrix).start()
        keep_copy(matrix).start()

    def z_copy(way, stage, matrix, given, device):
        block = chunk(matrix, given * 2, 2)
        return remote(
            block,
            block,
            z_send.at[way, stage, matrix],
            z_recv.at[way, stage, matrix],
            (device, tp),
        )

    def z_start(way, stage, matrix):
        given = z - stage if way == 0 else z + stage
        allowed = (given >= 0) & (z + 1 < slabs) if way == 0 else (given < slabs) & (z >= 1)

        @pl.when(allowed)
        def _():
            z_copy(way, stage, matrix, given, sp + 2 - 4 * way).start()

    def z_sent(way, stage, matrix):
        given = z - stage if way == 0 else z + stage
        allowed = (given >= 0) & (z + 1 < slabs) if way == 0 else (given < slabs) & (z >= 1)

        @pl.when(allowed)
        def _():
            z_copy(way, stage, matrix, given, sp + 2 - 4 * way).wait_send()

    def weights_start(matrix):
        keep_copy(matrix).wait()
        cross_wait(matrix)
        for way in range(2):
            z_start(way, 0, matrix)

    def origin_of(order):
        upper = z // 2
        return (z, z + 1 - 2 * (z % 2), 2 - upper, 3 - 3 * upper)[order]

    def z_from(way):
        return sp - 2 + 4 * way

    def weights_arrive(matrix, order):
        origin = origin_of(order)
        for way in range(2):
            for stage in range(slabs - 1):

                @pl.when((z - origin if way == 0 else origin - z) == stage + 1)
                def _():
                    z_copy(way, stage, matrix, origin, z_from(way)).wait_recv()
                    if stage + 2 < slabs:
                        z_start(way, stage + 1, matrix)

    def relays(place):
        for at, matrix, order in RELAYS:
            if at == place:

                @pl.when(inner)
                def _():
                    weights_arrive(matrix, order)

    def weights_end(matrix):
        @pl.when(jnp.logical_not(inner))
        def _():
            for order in range(1, slabs):
                weights_arrive(matrix, order)

    def back_copy(piece):
        return remote(
            outp.at[piece],
            att.at[pl.ds(sp * head_dim, head_dim), :],
            b_send.at[piece],
            b_recv.at[sp],
            (piece, tp),
        )

    def back_wait(source):
        remote(
            outp.at[source],
            att.at[pl.ds(source * head_dim, head_dim), :],
            b_send.at[source],
            b_recv.at[source],
            (source, tp),
        ).wait_recv()

    own_back = pltpu.make_async_copy(
        outp.at[sp], att.at[pl.ds(sp * head_dim, head_dim), :], own_sem.at[1]
    )

    def one_piece(index, carry):
        @pl.when(index == sp)
        def _():
            own_piece.wait()

        @pl.when(index != sp)
        def _():
            piece_wait(index)

        outp[index] = flash_piece(index, recv, kk, vaug, qaug, high_ref, acc_ref, head_dim)

        @pl.when(index == sp)
        def _():
            own_back.start()

        @pl.when(index != sp)
        def _():
            back_copy(index).start()

        @pl.when((index == START_AT) & (z + 1 < slabs))
        def _():
            for matrix in range(3):
                weights_start(matrix)

        for at in range(8):
            if any(relay[0] == at for relay in RELAYS):

                @pl.when(index == at)
                def _():
                    relays(at)

        return carry

    @pl.when(z + 1 == slabs)
    def _():
        for matrix in range(3):
            weights_start(matrix)

    lax.fori_loop(0, n_sp, one_piece, 0)

    own_back.wait()

    def wait_back(step, carry):
        back_wait((sp + step) % n_sp)
        return carry

    lax.fori_loop(1, n_sp, wait_back, 0)
    load_ow.wait()
    load_st.wait()
    attT[...] = att[...].T

    def mix_block(owner):
        return jnp.dot(
            attT[pl.ds(owner * rows, rows), :], owv[...], preferred_element_type=jnp.float32
        )

    def pair_copy(slot):
        return remote(psend.at[slot], precv.at[slot], p_send.at[slot], p_recv.at[slot], c_peer)

    def mix_away(slot, carry):
        psend[slot] = mix_block(((x + 1 + slot) % 2) * 2 + 1 - c).astype(jnp.bfloat16)
        pair_copy(slot).start()
        return carry

    lax.fori_loop(0, 2, mix_away, 0)

    def mix_own(slot, carry):
        pown[slot] = mix_block(((x + 1 + slot) % 2) * 2 + c)
        return carry

    lax.fori_loop(0, 2, mix_own, 0)
    pair_copy(0).wait_recv()
    xs[...] = (pown[0] + precv[0].astype(jnp.float32)).astype(jnp.bfloat16)
    across = remote(xs, xr, x_send.at[0], x_recv.at[0], x_peer)
    across.start()
    relays("across")
    pair_copy(1).wait_recv()
    across.wait_recv()

    def place(by, bx, bc):
        return ((y + by) % 2) * 4 + ((x + bx) % 2) * 2 + (c + bc) % 2

    own = place(0, 0, 0)
    tile = 16

    def norm(matrix, gain, shift):
        centred = matrix - jnp.mean(matrix, axis=-1, keepdims=True)
        spread = jnp.mean(centred * centred, axis=-1, keepdims=True)
        return (centred * lax.rsqrt(spread + EPSILON) * gain + shift).astype(jnp.bfloat16)

    def mix_norm(step, carry):
        at = pl.ds(pl.multiple_of(step * tile, tile), tile)
        summed = pown[1, at, :] + precv[1, at, :].astype(jnp.float32)
        summed = (summed + xr[at, :].astype(jnp.float32)).astype(jnp.bfloat16)
        nb[own, at, :] = norm(
            ALPHA * stv[at, :].astype(jnp.float32) + summed.astype(jnp.float32),
            mg_ref[...],
            mb_ref[...],
        )
        return carry

    lax.fori_loop(0, rows // tile, mix_norm, 0, unroll=2)

    top = pl.ds(0, rows // 2)
    bottom = pl.ds(rows // 2, rows // 2)

    def block_copy(sem, block, device):
        return remote(nb.at[block], nb.at[block], g_send.at[sem], g_recv.at[sem], device)

    def half_copy(sem, block, taken, device):
        view = nb.at[block, taken, :]
        return remote(view, view, g_send.at[sem], g_recv.at[sem], device)

    gathers = [
        block_copy(0, own, c_peer),
        block_copy(1, own, x_peer),
        block_copy(2, own, y_peer),
        half_copy(3, place(0, 1, 0), top, y_peer),
        half_copy(4, place(1, 0, 0), bottom, x_peer),
        block_copy(5, place(0, 1, 0), c_peer),
        block_copy(6, place(1, 0, 0), c_peer),
        block_copy(7, place(1, 1, 0), c_peer),
    ]
    arrivals = [
        block_copy(0, place(0, 0, 1), c_peer),
        block_copy(1, place(0, 1, 0), x_peer),
        block_copy(2, place(1, 0, 0), y_peer),
        half_copy(3, place(1, 1, 0), top, y_peer),
        half_copy(4, place(1, 1, 0), bottom, x_peer),
        block_copy(5, place(0, 1, 1), c_peer),
        block_copy(6, place(1, 0, 1), c_peer),
        block_copy(7, place(1, 1, 1), c_peer),
    ]
    gathers[1].start()
    gathers[2].start()
    gathers[0].start()
    relays("gather")

    def up_block(step):
        by, bx = step // 2, step % 2
        first = place(by, bx, 0) // 2
        block = nb[pl.ds(first * 2, 2)].reshape(2 * rows, width)
        contract = (((1,), (1,)), ((), ()))
        gate = lax.dot_general(block, wbuf[0], contract, preferred_element_type=jnp.float32)
        up = lax.dot_general(block, wbuf[1], contract, preferred_element_type=jnp.float32)
        hid[step] = (gate / (1.0 + jnp.exp(-gate)) * up).astype(jnp.bfloat16)

    arrivals[1].wait_recv()
    gathers[3].start()
    gathers[5].start()
    arrivals[2].wait_recv()
    gathers[4].start()
    gathers[6].start()
    arrivals[0].wait_recv()
    relays("gathered")
    weights_end(0)
    weights_end(1)

    def forward(step, carry):
        @pl.when(step == 1)
        def _():
            arrivals[5].wait_recv()

        @pl.when(step == 2)
        def _():
            arrivals[6].wait_recv()
            arrivals[3].wait_recv()
            arrivals[4].wait_recv()
            gathers[7].start()

        @pl.when(step == 3)
        def _():
            arrivals[7].wait_recv()

        up_block(step)
        return carry

    lax.fori_loop(0, 4, forward, 0)
    relays("upped")
    def span_of(origin, first, count):
        start = pl.multiple_of((origin * 2 + first) * cols, cols)
        return pl.ds(start, count * cols)

    def core_copy(step, origin):
        given = dsend.at[step, :, span_of(origin, 0, 2)]
        taken = drecv.at[step, :, span_of(origin, 0, 2)]
        return remote(given, taken, d_send.at[step, origin], d_recv.at[step, origin], c_peer)

    def out_copy(number, origin):
        slot, first, device = (
            (0, 0, x_peer),
            (1, 0, x_peer),
            (0, 1, y_peer),
            (2, 1, y_peer),
            (2, 0, y_peer),
            (1, 1, x_peer),
        )[number]
        return remote(
            rsb.at[slot, :, span_of(origin, first, 1)],
            r1.at[number, origin],
            r_send.at[number, origin],
            r_recv.at[number, origin],
            device,
        )

    def core_sum(step, origin):
        core_copy(step, origin).wait_recv()
        span = span_of(origin, 0, 2)
        summed = dacc[step, :, span] + drecv[step, :, span].astype(jnp.float32)
        dacc[step, :, span] = summed
        return summed.astype(jnp.bfloat16)

    def down_stage(stage, carry):
        upper = z // 2
        origin = jnp.where(stage == 1, z + 1 - 2 * (z % 2), 2 - upper)
        origin = jnp.where(stage == 0, z, jnp.where(stage == 3, 3 - 3 * upper, origin))

        for order in range(1, slabs):

            @pl.when((stage == order) & jnp.logical_not(inner))
            def _():
                weights_arrive(2, order)

        span = span_of(origin, 0, 2)

        def down_step(step, inner):
            slot = 3 - step
            slot = (slot // 2) + 2 * (slot % 2)
            given = hid[slot, pl.ds((1 - c) * rows, rows), :]
            dsend[step, :, span] = jnp.dot(
                given, wbuf[2, :, span], preferred_element_type=jnp.float32
            ).astype(jnp.bfloat16)
            core_copy(step, origin).start()
            kept = hid[slot, pl.ds(c * rows, rows), :]
            dacc[step, :, span] = jnp.dot(
                kept, wbuf[2, :, span], preferred_element_type=jnp.float32
            )
            return inner

        lax.fori_loop(0, 4, down_step, 0)
        rsb[0, :, span] = core_sum(0, origin)
        out_copy(0, origin).start()
        out_copy(2, origin).start()
        rsb[1, :, span_of(origin, 0, 1)] = core_sum(1, origin)[:, :cols]
        out_copy(1, origin).start()
        rsb[2, :, span_of(origin, 1, 1)] = core_sum(2, origin)[:, cols:]
        out_copy(3, origin).start()
        core_sum(3, origin)
        out_copy(0, origin).wait_recv()
        near = span_of(origin, 0, 1)
        rsb[2, :, near] = (dacc[2, :, near] + r1[0, origin].astype(jnp.float32)).astype(
            jnp.bfloat16
        )
        out_copy(4, origin).start()
        out_copy(2, origin).wait_recv()
        near = span_of(origin, 1, 1)
        rsb[1, :, near] = (dacc[1, :, near] + r1[2, origin].astype(jnp.float32)).astype(
            jnp.bfloat16
        )
        out_copy(5, origin).start()
        return carry

    lax.fori_loop(0, 4, down_stage, 0)
    for number in (1, 3, 4, 5):
        for origin in range(4):
            out_copy(number, origin).wait_recv()

    def last_norm(step, carry):
        at = pl.ds(pl.multiple_of(step * tile, tile), tile)
        terms = []
        for origin in range(4):
            for first, one, two in ((0, 1, 4), (1, 3, 5)):
                start = (origin * 2 + first) * cols
                terms.append(
                    dacc[3, at, start : start + cols]
                    + r1[one, origin, at, :].astype(jnp.float32)
                    + r1[two, origin, at, :].astype(jnp.float32)
                )
        lowered = jnp.concatenate(terms, axis=1).astype(jnp.bfloat16).astype(jnp.float32)
        out_ref[at, :] = norm(
            ALPHA * nb[own, at, :].astype(jnp.float32) + lowered, fg_ref[...], fb_ref[...]
        )
        return carry

    lax.fori_loop(0, rows // tile, last_norm, 0, unroll=2)

    def sent_pieces(step, carry):
        piece_copy((sp + step) % n_sp).wait_send()
        back_copy((sp + step) % n_sp).wait_send()
        return carry

    lax.fori_loop(1, n_sp, sent_pieces, 0)
    for matrix in range(3):
        cross_copy(matrix).wait_send()
        for way in range(2):
            for stage in range(slabs - 1):
                z_sent(way, stage, matrix)

    pair_copy(0).wait_send()
    pair_copy(1).wait_send()
    across.wait_send()
    for copy in gathers:
        copy.wait_send()
    for origin in range(4):
        for step in range(4):
            core_copy(step, origin).wait_send()
        for number in range(6):
            out_copy(number, origin).wait_send()


START_AT = 1
RELAYS = (
    (7, 0, 1),
    (7, 0, 2),
    ("across", 1, 1),
    ("across", 1, 2),
    ("gather", 0, 3),
    ("gathered", 1, 3),
    ("gathered", 2, 1),
    ("gathered", 2, 2),
    ("upped", 2, 3),
)


def whole_layer(
    queries,
    key_rows,
    value_rows,
    log_forget,
    stream_in,
    out_weight,
    mix_gain,
    mix_bias,
    gate_weight,
    up_weight,
    down_weight,
    ffn_gain,
    ffn_bias,
):
    length, row_width = queries.shape
    heads = log_forget.shape[1]
    head_dim = row_width // heads
    pieces = lax.axis_size("sp")
    slabs = pieces // 2
    rows = length // lax.axis_size("tp")
    width = stream_in.shape[1]
    cols, hidden = gate_weight.shape
    part = hidden // 2
    packed = pack_pieces(queries, key_rows, value_rows, log_forget)
    high_rows = packed.shape[1] - 2 * head_dim
    bf16, f32 = jnp.bfloat16, jnp.float32
    vmem, dma = pltpu.VMEM, pltpu.SemaphoreType.DMA
    scratch = [
        vmem((pieces,) + packed.shape[1:], bf16),
        vmem((pieces, length, 128), bf16),
        vmem((pieces, high_rows, length), bf16),
        vmem((128, length), bf16),
        vmem((1, length), f32),
        vmem((high_rows, length), f32),
        vmem((pieces, head_dim, length), bf16),
        vmem((row_width, length), bf16),
        vmem((length, row_width), bf16),
        vmem((2, hidden, cols), bf16),
        vmem((3, part, width), bf16),
        vmem((row_width, width), bf16),
        vmem((rows, width), bf16),
        vmem((2, rows, width), bf16),
        vmem((2, rows, width), bf16),
        vmem((2, rows, width), f32),
        vmem((rows, width), bf16),
        vmem((rows, width), bf16),
        vmem((8, rows, width), bf16),
        vmem((4, 2 * rows, part), bf16),
        vmem((4, rows, width), bf16),
        vmem((4, rows, width), bf16),
        vmem((4, rows, width), f32),
        vmem((3, rows, width), bf16),
        vmem((6, 4, rows, cols), bf16),
        dma((2,)),
        dma((2,)),
        dma((pieces,)),
        dma((pieces,)),
        dma((pieces,)),
        dma((pieces,)),
        dma((3,)),
        dma((3,)),
        dma((3,)),
        dma((2, slabs - 1, 3)),
        dma((2, slabs - 1, 3)),
        dma((2,)),
        dma((2,)),
        dma((1,)),
        dma((1,)),
        dma((8,)),
        dma((8,)),
        dma((4, 4)),
        dma((4, 4)),
        dma((6, 4)),
        dma((6, 4)),
    ]
    in_vmem = pl.BlockSpec(memory_space=pltpu.VMEM)
    anywhere = pl.BlockSpec(memory_space=pl.ANY)
    return pl.pallas_call(
        layer_kernel,
        out_shape=jax.ShapeDtypeStruct((rows, width), bf16),
        in_specs=[anywhere, in_vmem, in_vmem, anywhere, anywhere, anywhere] + [in_vmem] * 4,
        out_specs=in_vmem,
        scratch_shapes=scratch,
        compiler_params=pltpu.CompilerParams(
            vmem_limit_bytes=67043328, has_side_effects=True, collective_id=0
        ),
    )(
        packed,
        gate_weight,
        up_weight,
        down_weight,
        out_weight,
        stream_in,
        mix_gain[None, :],
        mix_bias[None, :],
        ffn_gain[None, :],
        ffn_bias[None, :],
    )


def swap_cores(block):
    count = lax.axis_size("tp")
    return lax.ppermute(block, "tp", [(i, i ^ 1) for i in range(count)])


def swap_across(block):
    count = lax.axis_size("tp")
    return lax.ppermute(block, "tp", [(i, i ^ 2) for i in range(count)])


def body(
    queries,
    key_rows,
    value_rows,
    log_forget,
    stream_in,
    out_weight,
    mix_gain,
    mix_bias,
    gate_weight,
    up_weight,
    down_weight,
    ffn_gain,
    ffn_bias,
):
    length = queries.shape[0]
    heads = log_forget.shape[1]
    head_dim = queries.shape[1] // heads
    pieces, group = lax.axis_size("sp"), lax.axis_size("tp")
    by_head = heads == pieces and head_dim + 16 <= 128 and head_dim % 16 == 0
    if by_head and pieces == 8 and group == 4:
        return whole_layer(
            queries,
            key_rows,
            value_rows,
            log_forget,
            stream_in,
            out_weight,
            mix_gain,
            mix_bias,
            gate_weight,
            up_weight,
            down_weight,
            ffn_gain,
            ffn_bias,
        )
    gate_full = lax.all_gather(gate_weight, "sp", axis=0, tiled=True)
    up_full = lax.all_gather(up_weight, "sp", axis=0, tiled=True)
    down_full = lax.all_gather(down_weight, "sp", axis=1, tiled=True)
    turned = attend(queries, key_rows, value_rows, log_forget).T
    own_rows = length // lax.axis_size("tp")
    offset = lax.axis_index("tp") * own_rows
    two_level = lax.axis_size("tp") == 4
    partial_mix = lax.dot_general(
        turned, out_weight, (((0,), (0,)), ((), ())), preferred_element_type=jnp.float32
    ).astype(jnp.bfloat16)
    if two_level:
        core = lax.axis_index("tp") % 2
        across = lax.axis_index("tp") // 2
        split = partial_mix.reshape(2, 2, own_rows, -1)
        mine = lax.dynamic_index_in_dim(split, core, 1, keepdims=False)
        other = lax.dynamic_index_in_dim(split, 1 - core, 1, keepdims=False)
        both = mine.astype(jnp.float32) + swap_cores(other).astype(jnp.float32)
        own = lax.dynamic_index_in_dim(both, across, 0, keepdims=False)
        away = lax.dynamic_index_in_dim(both, 1 - across, 0, keepdims=False)
        summed = (own + swap_across(away.astype(jnp.bfloat16)).astype(jnp.float32)).astype(
            jnp.bfloat16
        )
    else:
        summed = lax.psum_scatter(partial_mix, "tp", scatter_dimension=0, tiled=True)
    mix_out = lax.optimization_barrier(summed).astype(jnp.float32)
    stream_own = lax.dynamic_slice_in_dim(stream_in, offset, own_rows, 0)
    normed = layer_norm(
        ALPHA * stream_own.astype(jnp.float32) + mix_out, mix_gain, mix_bias
    ).astype(jnp.bfloat16)
    if two_level:
        pair = jnp.concatenate([normed, swap_across(normed)], axis=0)
        gathered = jnp.concatenate([pair, swap_cores(pair)], axis=0)
    else:
        gathered = lax.all_gather(normed, "tp", axis=0, tiled=True)
    gate_part = jnp.dot(gathered, gate_full, preferred_element_type=jnp.float32)
    up_part = jnp.dot(gathered, up_full, preferred_element_type=jnp.float32)
    hidden = (jax.nn.silu(gate_part) * up_part).astype(jnp.bfloat16)
    if two_level:
        columns = []
        half = down_full.shape[1] // 2
        for start in (0, half):
            terms = jnp.dot(
                hidden, down_full[:, start : start + half], preferred_element_type=jnp.float32
            ).astype(jnp.bfloat16)
            both = terms[: 2 * own_rows].astype(jnp.float32) + swap_cores(
                terms[2 * own_rows :]
            ).astype(jnp.float32)
            columns.append(
                both[:own_rows]
                + swap_across(both[own_rows:].astype(jnp.bfloat16)).astype(jnp.float32)
            )
        lowered = jnp.concatenate(columns, axis=1)
    else:
        partial_terms = jnp.dot(hidden, down_full, preferred_element_type=jnp.float32)
        lowered = lax.psum_scatter(
            partial_terms.astype(jnp.bfloat16), "tp", scatter_dimension=0, tiled=True
        ).astype(jnp.float32)
    lowered = lax.optimization_barrier(lowered.astype(jnp.bfloat16)).astype(jnp.float32)
    result = layer_norm(ALPHA * normed.astype(jnp.float32) + lowered, ffn_gain, ffn_bias)
    return result.astype(jnp.bfloat16)


def solution(mesh):
    placed = (
        P("sp", "tp"),
        P("sp", "tp"),
        P("sp", "tp"),
        P("sp", "tp"),
        P("sp", None),
        P("tp", None),
        P(),
        P(),
        P("sp", "tp"),
        P("sp", "tp"),
        P("tp", "sp"),
        P(),
        P(),
    )
    return jax.shard_map(
        body, mesh=mesh, in_specs=placed, out_specs=P(("sp", "tp"), None), check_vma=False
    )
```

```python
import jax
import jax.numpy as jnp
from jax import lax
from jax.experimental import pallas as pl
from jax.experimental.pallas import tpu as pltpu
from jax.sharding import PartitionSpec as P


ALPHA = 8.0**0.25
EPSILON = 1e-05


def layer_norm(matrix, norm_gain, norm_shift):
    centred = matrix - jnp.mean(matrix, axis=-1, keepdims=True)
    spread = jnp.mean(centred * centred, axis=-1, keepdims=True)
    return centred * lax.rsqrt(spread + EPSILON) * norm_gain + norm_shift


def attend(queries, key_rows, value_rows, log_forget):
    length, row_width = queries.shape
    head_count = log_forget.shape[1]
    head_dim = row_width // head_count
    score_scale = head_dim ** (-0.5)
    first_pos = lax.axis_index("sp") * length
    last_pos = first_pos + length
    query_heads = queries.reshape(length, head_count, head_dim)
    query_gates = log_forget.T
    query_pos = first_pos + jnp.arange(length, dtype=jnp.int32)
    gates_all = lax.all_gather(log_forget, "sp", axis=0, tiled=True)
    initial = (
        jnp.full((head_count, length), -1e30, jnp.float32),
        jnp.zeros((head_count, length), jnp.float32),
        jnp.zeros((length, head_count, head_dim), jnp.float32),
    )
    running = initial
    key_piece = lax.all_gather(key_rows, "sp", axis=0, tiled=True)
    value_piece = lax.all_gather(value_rows, "sp", axis=0, tiled=True)
    piece_len = key_piece.shape[0]
    shards = piece_len // length
    group_size = max(
        [
            count_try
            for count_try in range(1, shards + 1)
            if shards % count_try == 0 and count_try * length <= max(length, 512)
        ]
    )
    block_len = group_size * length
    blocks = piece_len // block_len
    key_blocks = key_piece.reshape(blocks, block_len, head_count, head_dim)
    value_blocks = value_piece.reshape(blocks, block_len, head_count, head_dim)
    gate_blocks = gates_all.reshape(blocks, block_len, head_count)
    block_starts = block_len * jnp.arange(blocks, dtype=jnp.int32)

    def one_block(running_state, packed):
        key_block, value_block, gate_block, block_start = packed

        def compute(state_in):
            highest, totals, weighted = state_in
            scores = (
                jnp.einsum(
                    "qhd,khd->hqk", query_heads, key_block, preferred_element_type=jnp.float32
                )
                * score_scale
            )
            scores = scores + query_gates[:, :, None] - gate_block.T[:, None, :]
            key_pos = block_start + jnp.arange(block_len, dtype=jnp.int32)
            allowed = (key_pos[None, :] <= query_pos[:, None])[None]
            masked = jnp.where(allowed, scores, -1e30)
            new_high = jnp.maximum(highest, jnp.max(masked, axis=2))
            weights = jnp.where(allowed, jnp.exp(masked - new_high[:, :, None]), 0.0)
            factor = jnp.exp(highest - new_high)
            totals = totals * factor + jnp.sum(weights, axis=2)
            weighted = weighted * factor.T[:, :, None] + jnp.einsum(
                "hqk,khd->qhd",
                weights.astype(jnp.bfloat16),
                value_block,
                preferred_element_type=jnp.float32,
            )
            return (new_high, totals, weighted)

        def keep_state(state_in):
            return state_in

        return (lax.cond(block_start < last_pos, compute, keep_state, running_state), None)

    running, unused = lax.scan(
        one_block, running, (key_blocks, value_blocks, gate_blocks, block_starts)
    )
    highest, totals, weighted = running
    return (weighted / totals.T[:, :, None]).reshape(length, row_width).astype(jnp.bfloat16)


SUB = 256


def gate_pieces(log_forget):
    gates = log_forget.T
    high = lax.reduce_precision(gates, 8, 7)
    middle = lax.reduce_precision(gates - high, 8, 7)
    low = gates - high - middle
    rows = jnp.stack([high, middle, low], axis=1).astype(jnp.bfloat16)
    return jnp.pad(rows, ((0, 0), (0, 13), (0, 0)))


def flash_piece(index, recv, kk, vaug, qaug, high_ref, acc_ref, head_dim):
    length = recv.shape[2]
    sub = SUB if length % SUB == 0 else length
    scale = head_dim**-0.5
    gate_rows = recv.shape[1] - 3 * head_dim
    query_at = head_dim + gate_rows
    value_at = query_at + head_dim
    kk[index] = recv[index, 0:128, :].T
    vaug[index, 0:head_dim, :] = recv[index, value_at : value_at + head_dim, :]
    row_index = lax.broadcasted_iota(jnp.int32, (gate_rows, length), 0)
    vaug[index, head_dim : head_dim + gate_rows, :] = jnp.where(row_index < 1, 1.0, 0.0).astype(
        jnp.bfloat16
    )
    block = recv[index, query_at : query_at + head_dim, :]
    qaug[0:head_dim, :] = (block.astype(jnp.float32) * scale).astype(jnp.bfloat16)
    qaug[head_dim : head_dim + gate_rows, :] = jnp.where(row_index < 3, -1.0, 0.0).astype(
        jnp.bfloat16
    )
    qaug[head_dim + gate_rows : 128, :] = jnp.zeros(
        (128 - head_dim - gate_rows, length), jnp.bfloat16
    )
    high_ref[...] = jnp.full_like(high_ref, -1e30)
    acc_ref[...] = jnp.zeros_like(acc_ref)

    def pair(piece, diagonal):
        starts = range(0, length, sub)
        spans = [slice(start, start + sub) for start in starts]
        widths = [start + sub if diagonal else length for start in starts]
        all_scores = [
            jnp.dot(kk[piece, 0:width, :], qaug[:, span], preferred_element_type=jnp.float32)
            for span, width in zip(spans, widths)
        ]
        if diagonal:
            key_pos = lax.broadcasted_iota(jnp.int32, (sub, sub), 0)
            allowed = key_pos <= lax.broadcasted_iota(jnp.int32, (sub, sub), 1)
            cut = [jnp.where(allowed, scores[-sub:], -1e30) for scores in all_scores]
            all_scores = cut[:1] + [
                jnp.concatenate([scores[:-sub], last], axis=0)
                for scores, last in zip(all_scores[1:], cut[1:])
            ]
        for scores, span, width in zip(all_scores, spans, widths):
            old_high = high_ref[:, span]
            new_high = jnp.maximum(old_high, jnp.max(scores, axis=0, keepdims=True))
            weights = jnp.exp(scores - new_high).astype(jnp.bfloat16)
            factor = jnp.exp(old_high - new_high)
            high_ref[:, span] = new_high
            acc_ref[:, span] = acc_ref[:, span] * factor + jnp.dot(
                vaug[piece, :, 0:width], weights, preferred_element_type=jnp.float32
            )

    def earlier(piece, inner):
        pair(piece, False)
        return inner

    lax.fori_loop(0, index, earlier, 0)
    pair(index, True)
    return (acc_ref[0:head_dim, :] / acc_ref[head_dim : head_dim + 1, :]).astype(jnp.bfloat16)


def layer_kernel(
    q_ref,
    k_ref,
    v_ref,
    t_ref,
    g_ref,
    u_ref,
    d_ref,
    ow_ref,
    st_ref,
    mg_ref,
    mb_ref,
    fg_ref,
    fb_ref,
    out_ref,
    packed,
    recv,
    kk,
    vaug,
    qaug,
    high_ref,
    acc_ref,
    outp,
    att,
    attT,
    wt,
    wbuf,
    owv,
    stv,
    psend,
    precv,
    xs,
    xr,
    nb,
    hid,
    dsend,
    drecv,
    dacc,
    rsb,
    r1,
    local_sem,
    own_sem,
    a_send,
    a_recv,
    b_send,
    b_recv,
    y_send,
    y_recv,
    w_sem,
    z_send,
    z_recv,
    p_send,
    p_recv,
    x_send,
    x_recv,
    g_send,
    g_recv,
    d_send,
    d_recv,
    r_send,
    r_recv,
):
    n_sp = lax.axis_size("sp")
    sp = lax.axis_index("sp")
    tp = lax.axis_index("tp")
    z, y = sp // 2, sp % 2
    x, c = tp // 2, tp % 2
    slabs = n_sp // 2
    y_peer = (z * 2 + 1 - y, tp)
    x_peer = (sp, (1 - x) * 2 + c)
    c_peer = (sp, x * 2 + 1 - c)
    length = recv.shape[2]
    head_dim = outp.shape[1]
    rows = out_ref.shape[0]
    width = out_ref.shape[1]
    part = wt.shape[1] // 2
    cols = wt.shape[2]

    def remote(src, dst, send, receive, device):
        return pltpu.make_async_remote_copy(
            src_ref=src,
            dst_ref=dst,
            send_sem=send,
            recv_sem=receive,
            device_id=device,
            device_id_type=pl.DeviceIdType.MESH,
        )

    barrier = pltpu.get_barrier_semaphore()

    def greet(step, carry):
        pl.semaphore_signal(
            barrier,
            inc=1,
            device_id=((sp + step) % n_sp, tp),
            device_id_type=pl.DeviceIdType.MESH,
        )
        return carry

    lax.fori_loop(1, n_sp, greet, 0)
    for device in (x_peer, c_peer):
        pl.semaphore_signal(
            barrier, inc=1, device_id=device, device_id_type=pl.DeviceIdType.MESH
        )
    gate_rows = t_ref.shape[1]
    packed[:, head_dim : head_dim + gate_rows, :] = t_ref[...]
    for first, rows_ref in (
        (0, k_ref),
        (head_dim + gate_rows, q_ref),
        (2 * head_dim + gate_rows, v_ref),
    ):
        turned = rows_ref[...].T
        packed[:, first : first + head_dim, :] = turned.reshape(n_sp, head_dim, length)
    wt[0] = g_ref[...].T
    wt[1] = u_ref[...].T
    pl.semaphore_wait(barrier, n_sp + 1)

    def piece_copy(other):
        return remote(
            packed.at[other], recv.at[sp], a_send.at[other], a_recv.at[sp], (other, tp)
        )

    def piece_wait(source):
        remote(
            packed.at[source], recv.at[source], a_send.at[source], a_recv.at[source], (source, tp)
        ).wait_recv()

    own_piece = pltpu.make_async_copy(packed.at[sp], recv.at[sp], own_sem.at[0])
    own_piece.start()

    def send_piece(step, carry):
        piece_copy((sp + n_sp - step) % n_sp).start()
        return carry

    lax.fori_loop(1, n_sp, send_piece, 0)
    load_ow = pltpu.make_async_copy(ow_ref, owv, local_sem.at[0])
    load_st = pltpu.make_async_copy(st_ref.at[pl.ds(tp * rows, rows), :], stv, local_sem.at[1])
    load_ow.start()
    load_st.start()

    inner = (z > 0) & (z + 1 < slabs)

    def chunk(matrix, owner, count):
        return wbuf.at[matrix, :, pl.ds(pl.multiple_of(owner * cols, cols), count * cols)]

    def weight_rows(matrix, which):
        taken = pl.ds(which * part, part)
        return d_ref.at[taken, :] if matrix == 2 else wt.at[matrix, taken, :]

    def keep_copy(matrix):
        return pltpu.make_async_copy(
            weight_rows(matrix, y), chunk(matrix, sp, 1), w_sem.at[matrix]
        )

    def cross_copy(matrix):
        return remote(
            weight_rows(matrix, 1 - y),
            chunk(matrix, sp, 1),
            y_send.at[matrix],
            y_recv.at[matrix],
            y_peer,
        )

    def cross_wait(matrix):
        block = chunk(matrix, z * 2 + 1 - y, 1)
        remote(block, block, y_send.at[matrix], y_recv.at[matrix], y_peer).wait_recv()

    for matrix in range(2):
        cross_copy(matrix).start()
        keep_copy(matrix).start()
    keep_copy(2).start()

    def z_copy(way, stage, matrix, given, device):
        block = chunk(matrix, given * 2, 2)
        return remote(
            block,
            block,
            z_send.at[way, stage, matrix],
            z_recv.at[way, stage, matrix],
            (device, tp),
        )

    def z_start(way, stage, matrix, also=True):
        given = z - stage if way == 0 else z + stage
        allowed = (given >= 0) & (z + 1 < slabs) if way == 0 else (given < slabs) & (z >= 1)
        allowed = allowed & also

        @pl.when(allowed)
        def _():
            z_copy(way, stage, matrix, given, sp + 2 - 4 * way).start()

    def z_sent(way, stage, matrix):
        given = z - stage if way == 0 else z + stage
        allowed = (given >= 0) & (z + 1 < slabs) if way == 0 else (given < slabs) & (z >= 1)

        @pl.when(allowed)
        def _():
            z_copy(way, stage, matrix, given, sp + 2 - 4 * way).wait_send()

    def halves_ready(matrix):
        keep_copy(matrix).wait()
        part_start(matrix, y)

    def inward_start(matrix, also=True):
        for way in range(2):
            z_start(way, 0, matrix, (z // 2 == way) & also)

    def part_start(matrix, column):
        for way in range(2):
            device = sp + 2 - 4 * way

            @pl.when(inner & (z // 2 != way))
            def _():
                block = chunk(matrix, z * 2 + column, 1)
                remote(
                    block,
                    block,
                    z_send.at[way, 0, matrix],
                    z_recv.at[way, 0, matrix],
                    (device, tp),
                ).start()

    def weights_start():
        halves_ready(0)
        halves_ready(1)
        halves_ready(2)
        cross_wait(0)
        inward_start(0)
        part_start(0, 1 - y)
        cross_wait(1)
        inward_start(1, z != 1)
        part_start(1, 1 - y)

    def origin_of(order):
        upper = z // 2
        return (z, z + 1 - 2 * (z % 2), 2 - upper, 3 - 3 * upper)[order]

    def z_from(way):
        return sp - 2 + 4 * way

    def weights_arrive(matrix, order):
        origin = origin_of(order)
        for way in range(2):
            for stage in range(slabs - 1):

                @pl.when((z - origin if way == 0 else origin - z) == stage + 1)
                def _():
                    z_copy(way, stage, matrix, origin, z_from(way)).wait_recv()
                    if stage + 2 < slabs:
                        z_start(way, stage + 1, matrix)

    def relays(place):
        for at, slab, matrix, order in RELAYS:
            if at == place:

                @pl.when(inner if slab is None else z == slab)
                def _():
                    weights_arrive(matrix, order)

    def weights_end(matrix):
        @pl.when(jnp.logical_not(inner))
        def _():
            for order in range(1, slabs):
                weights_arrive(matrix, order)

    def back_copy(piece):
        return remote(
            outp.at[piece],
            att.at[pl.ds(sp * head_dim, head_dim), :],
            b_send.at[piece],
            b_recv.at[sp],
            (piece, tp),
        )

    def back_wait(source):
        remote(
            outp.at[source],
            att.at[pl.ds(source * head_dim, head_dim), :],
            b_send.at[source],
            b_recv.at[source],
            (source, tp),
        ).wait_recv()

    own_back = pltpu.make_async_copy(
        outp.at[sp], att.at[pl.ds(sp * head_dim, head_dim), :], own_sem.at[1]
    )

    def one_piece(index, carry):
        @pl.when(index == sp)
        def _():
            own_piece.wait()

        @pl.when(index != sp)
        def _():
            piece_wait(index)

        outp[index] = flash_piece(index, recv, kk, vaug, qaug, high_ref, acc_ref, head_dim)

        @pl.when(index == sp)
        def _():
            own_back.start()

        @pl.when(index != sp)
        def _():
            back_copy(index).start()

        @pl.when((index == START_AT) & (z == 0))
        def _():
            weights_start()

        @pl.when(index == CROSS_AT)
        def _():
            cross_copy(2).start()

        @pl.when(index == DOWN_AT)
        def _():
            cross_wait(2)
            part_start(2, 1 - y)

        for at in range(8):
            if any(relay[0] == at for relay in RELAYS):

                @pl.when(index == at)
                def _():
                    relays(at)

        return carry

    @pl.when(z > 0)
    def _():
        weights_start()

    lax.fori_loop(0, n_sp, one_piece, 0)
    inward_start(1, z == 1)
    relays("looped")
    inward_start(2)

    own_back.wait()

    def wait_back(step, carry):
        back_wait((sp + step) % n_sp)
        return carry

    lax.fori_loop(1, n_sp, wait_back, 0)
    load_ow.wait()
    load_st.wait()
    attT[...] = att[...].T

    def mix_block(owner):
        return jnp.dot(
            attT[pl.ds(owner * rows, rows), :], owv[...], preferred_element_type=jnp.float32
        )

    def pair_copy(slot):
        return remote(psend.at[slot], precv.at[slot], p_send.at[slot], p_recv.at[slot], c_peer)

    def mix_away(slot, carry):
        psend[slot] = mix_block(((x + 1 + slot) % 2) * 2 + 1 - c).astype(jnp.bfloat16)
        pair_copy(slot).start()
        return carry

    lax.fori_loop(0, 2, mix_away, 0)

    def mix_own(slot, carry):
        dacc[slot] = mix_block(((x + 1 + slot) % 2) * 2 + c)
        return carry

    lax.fori_loop(0, 2, mix_own, 0)
    pair_copy(0).wait_recv()
    xs[...] = (dacc[0] + precv[0].astype(jnp.float32)).astype(jnp.bfloat16)
    across = remote(xs, xr, x_send.at[0], x_recv.at[0], x_peer)
    across.start()
    relays("across")
    pair_copy(1).wait_recv()
    across.wait_recv()

    def place(by, bx, bc):
        return ((y + by) % 2) * 4 + ((x + bx) % 2) * 2 + (c + bc) % 2

    own = place(0, 0, 0)
    tile = 16

    def norm(matrix, gain, shift):
        centred = matrix - jnp.mean(matrix, axis=-1, keepdims=True)
        spread = jnp.mean(centred * centred, axis=-1, keepdims=True)
        return (centred * lax.rsqrt(spread + EPSILON) * gain + shift).astype(jnp.bfloat16)

    def mix_norm(step, carry):
        at = pl.ds(pl.multiple_of(step * tile, tile), tile)
        summed = dacc[1, at, :] + precv[1, at, :].astype(jnp.float32)
        summed = (summed + xr[at, :].astype(jnp.float32)).astype(jnp.bfloat16)
        nb[own, at, :] = norm(
            ALPHA * stv[at, :].astype(jnp.float32) + summed.astype(jnp.float32),
            mg_ref[...],
            mb_ref[...],
        )
        return carry

    lax.fori_loop(0, rows // tile, mix_norm, 0, unroll=2)

    top = pl.ds(0, rows // 2)
    bottom = pl.ds(rows // 2, rows // 2)

    def block_copy(sem, block, device):
        return remote(nb.at[block], nb.at[block], g_send.at[sem], g_recv.at[sem], device)

    def half_copy(sem, block, taken, device):
        view = nb.at[block, taken, :]
        return remote(view, view, g_send.at[sem], g_recv.at[sem], device)

    gathers = [
        block_copy(0, own, c_peer),
        block_copy(1, own, x_peer),
        block_copy(2, own, y_peer),
        half_copy(3, place(0, 1, 0), top, y_peer),
        half_copy(4, place(1, 0, 0), bottom, x_peer),
        block_copy(5, place(0, 1, 0), c_peer),
        block_copy(6, place(1, 0, 0), c_peer),
        block_copy(7, place(1, 1, 0), c_peer),
    ]
    arrivals = [
        block_copy(0, place(0, 0, 1), c_peer),
        block_copy(1, place(0, 1, 0), x_peer),
        block_copy(2, place(1, 0, 0), y_peer),
        half_copy(3, place(1, 1, 0), top, y_peer),
        half_copy(4, place(1, 1, 0), bottom, x_peer),
        block_copy(5, place(0, 1, 1), c_peer),
        block_copy(6, place(1, 0, 1), c_peer),
        block_copy(7, place(1, 1, 1), c_peer),
    ]
    gathers[1].start()
    gathers[2].start()
    gathers[0].start()
    relays("gather")

    def up_block(step):
        by, bx = step // 2, step % 2
        first = place(by, bx, 0) // 2
        block = nb[pl.ds(first * 2, 2)].reshape(2 * rows, width)
        contract = (((1,), (1,)), ((), ()))
        gate = lax.dot_general(block, wbuf[0], contract, preferred_element_type=jnp.float32)
        up = lax.dot_general(block, wbuf[1], contract, preferred_element_type=jnp.float32)
        hid[step] = (gate / (1.0 + jnp.exp(-gate)) * up).astype(jnp.bfloat16)

    arrivals[1].wait_recv()
    gathers[3].start()
    gathers[5].start()
    arrivals[2].wait_recv()
    gathers[4].start()
    gathers[6].start()
    arrivals[0].wait_recv()
    relays("gathered")
    weights_end(0)
    weights_end(1)

    def forward(step, carry):
        @pl.when(step == 1)
        def _():
            arrivals[5].wait_recv()

        @pl.when(step == 2)
        def _():
            arrivals[6].wait_recv()
            arrivals[3].wait_recv()
            arrivals[4].wait_recv()
            gathers[7].start()

        @pl.when(step == 3)
        def _():
            arrivals[7].wait_recv()

        up_block(step)
        return carry

    lax.fori_loop(0, 4, forward, 0)
    relays("upped")
    def span_of(origin, first, count):
        start = pl.multiple_of((origin * 2 + first) * cols, cols)
        return pl.ds(start, count * cols)

    def core_copy(step, origin):
        given = dsend.at[step, :, span_of(origin, 0, 2)]
        taken = drecv.at[step, :, span_of(origin, 0, 2)]
        return remote(given, taken, d_send.at[step, origin], d_recv.at[step, origin], c_peer)

    def out_copy(number, origin):
        slot, first, device = (
            (0, 0, x_peer),
            (1, 0, x_peer),
            (0, 1, y_peer),
            (2, 1, y_peer),
            (2, 0, y_peer),
            (1, 1, x_peer),
        )[number]
        return remote(
            rsb.at[slot, :, span_of(origin, first, 1)],
            r1.at[number, origin],
            r_send.at[number, origin],
            r_recv.at[number, origin],
            device,
        )

    def core_sum(step, origin):
        core_copy(step, origin).wait_recv()
        span = span_of(origin, 0, 2)
        summed = dacc[step, :, span] + drecv[step, :, span].astype(jnp.float32)
        dacc[step, :, span] = summed
        return summed.astype(jnp.bfloat16)

    def second_level(origin):
        out_copy(0, origin).wait_recv()
        near = span_of(origin, 0, 1)
        rsb[2, :, near] = (dacc[2, :, near] + r1[0, origin].astype(jnp.float32)).astype(
            jnp.bfloat16
        )
        out_copy(4, origin).start()
        out_copy(2, origin).wait_recv()
        near = span_of(origin, 1, 1)
        rsb[1, :, near] = (dacc[1, :, near] + r1[2, origin].astype(jnp.float32)).astype(
            jnp.bfloat16
        )
        out_copy(5, origin).start()

    def stage_origin(stage):
        upper = z // 2
        origin = jnp.where(stage == 1, z + 1 - 2 * (z % 2), 2 - upper)
        return jnp.where(stage == 0, z, jnp.where(stage == 3, 3 - 3 * upper, origin))

    def down_stage(stage, carry):
        origin = stage_origin(stage)

        for order in range(1, slabs):

            @pl.when((stage == order) & jnp.logical_not(inner))
            def _():
                weights_arrive(2, order)

        span = span_of(origin, 0, 2)

        def down_step(step, inner):
            slot = 3 - step
            slot = (slot // 2) + 2 * (slot % 2)
            given = hid[slot, pl.ds((1 - c) * rows, rows), :]
            dsend[step, :, span] = jnp.dot(
                given, wbuf[2, :, span], preferred_element_type=jnp.float32
            ).astype(jnp.bfloat16)
            core_copy(step, origin).start()
            kept = hid[slot, pl.ds(c * rows, rows), :]
            dacc[step, :, span] = jnp.dot(
                kept, wbuf[2, :, span], preferred_element_type=jnp.float32
            )
            return inner

        lax.fori_loop(0, 4, down_step, 0)

        @pl.when(stage > 0)
        def _():
            second_level(stage_origin(stage - 1))

        rsb[0, :, span] = core_sum(0, origin)
        out_copy(0, origin).start()
        out_copy(2, origin).start()
        rsb[1, :, span_of(origin, 0, 1)] = core_sum(1, origin)[:, :cols]
        out_copy(1, origin).start()
        rsb[2, :, span_of(origin, 1, 1)] = core_sum(2, origin)[:, cols:]
        out_copy(3, origin).start()
        core_sum(3, origin)
        return carry

    lax.fori_loop(0, 4, down_stage, 0)
    second_level(stage_origin(3))
    for number in (1, 3, 4, 5):
        for origin in range(4):
            out_copy(number, origin).wait_recv()

    def last_norm(step, carry):
        at = pl.ds(pl.multiple_of(step * tile, tile), tile)
        terms = []
        for origin in range(4):
            for first, one, two in ((0, 1, 4), (1, 3, 5)):
                start = (origin * 2 + first) * cols
                terms.append(
                    dacc[3, at, start : start + cols]
                    + r1[one, origin, at, :].astype(jnp.float32)
                    + r1[two, origin, at, :].astype(jnp.float32)
                )
        lowered = jnp.concatenate(terms, axis=1).astype(jnp.bfloat16).astype(jnp.float32)
        out_ref[at, :] = norm(
            ALPHA * nb[own, at, :].astype(jnp.float32) + lowered, fg_ref[...], fb_ref[...]
        )
        return carry

    lax.fori_loop(0, rows // tile, last_norm, 0, unroll=2)

    def sent_pieces(step, carry):
        piece_copy((sp + step) % n_sp).wait_send()
        back_copy((sp + step) % n_sp).wait_send()
        return carry

    lax.fori_loop(1, n_sp, sent_pieces, 0)
    for matrix in range(3):
        cross_copy(matrix).wait_send()
        for way in range(2):
            for stage in range(slabs - 1):
                z_sent(way, stage, matrix)

    pair_copy(0).wait_send()
    pair_copy(1).wait_send()
    across.wait_send()
    for copy in gathers:
        copy.wait_send()
    for origin in range(4):
        for step in range(4):
            core_copy(step, origin).wait_send()
        for number in range(6):
            out_copy(number, origin).wait_send()


START_AT = 2
CROSS_AT = 2
DOWN_AT = 6
RELAYS = (
    (5, 2, 0, 1),
    (5, 1, 0, 2),
    (7, None, 1, 2),
    ("looped", 1, 0, 1),
    (6, 2, 0, 2),
    ("looped", None, 1, 1),
    ("across", None, 0, 3),
    ("across", None, 2, 1),
    ("gather", None, 1, 3),
    ("gathered", None, 2, 2),
    ("upped", None, 2, 3),
)


def whole_layer(
    queries,
    key_rows,
    value_rows,
    log_forget,
    stream_in,
    out_weight,
    mix_gain,
    mix_bias,
    gate_weight,
    up_weight,
    down_weight,
    ffn_gain,
    ffn_bias,
):
    length, row_width = queries.shape
    heads = log_forget.shape[1]
    head_dim = row_width // heads
    pieces = lax.axis_size("sp")
    slabs = pieces // 2
    rows = length // lax.axis_size("tp")
    width = stream_in.shape[1]
    cols, hidden = gate_weight.shape
    part = hidden // 2
    gates = gate_pieces(log_forget)
    high_rows = head_dim + gates.shape[1]
    bf16, f32 = jnp.bfloat16, jnp.float32
    vmem, dma = pltpu.VMEM, pltpu.SemaphoreType.DMA
    scratch = [
        vmem((pieces, high_rows + 2 * head_dim, length), bf16),
        vmem((pieces, high_rows + 2 * head_dim, length), bf16),
        vmem((pieces, length, 128), bf16),
        vmem((pieces, high_rows, length), bf16),
        vmem((128, length), bf16),
        vmem((1, length), f32),
        vmem((high_rows, length), f32),
        vmem((pieces, head_dim, length), bf16),
        vmem((row_width, length), bf16),
        vmem((length, row_width), bf16),
        vmem((2, hidden, cols), bf16),
        vmem((3, part, width), bf16),
        vmem((row_width, width), bf16),
        vmem((rows, width), bf16),
        vmem((2, rows, width), bf16),
        vmem((2, rows, width), bf16),
        vmem((rows, width), bf16),
        vmem((rows, width), bf16),
        vmem((8, rows, width), bf16),
        vmem((4, 2 * rows, part), bf16),
        vmem((4, rows, width), bf16),
        vmem((4, rows, width), bf16),
        vmem((4, rows, width), f32),
        vmem((3, rows, width), bf16),
        vmem((6, 4, rows, cols), bf16),
        dma((2,)),
        dma((2,)),
        dma((pieces,)),
        dma((pieces,)),
        dma((pieces,)),
        dma((pieces,)),
        dma((3,)),
        dma((3,)),
        dma((3,)),
        dma((2, slabs - 1, 3)),
        dma((2, slabs - 1, 3)),
        dma((2,)),
        dma((2,)),
        dma((1,)),
        dma((1,)),
        dma((8,)),
        dma((8,)),
        dma((4, 4)),
        dma((4, 4)),
        dma((6, 4)),
        dma((6, 4)),
    ]
    in_vmem = pl.BlockSpec(memory_space=pltpu.VMEM)
    anywhere = pl.BlockSpec(memory_space=pl.ANY)
    return pl.pallas_call(
        layer_kernel,
        out_shape=jax.ShapeDtypeStruct((rows, width), bf16),
        in_specs=[in_vmem] * 6 + [anywhere] * 3 + [in_vmem] * 4,
        out_specs=in_vmem,
        scratch_shapes=scratch,
        compiler_params=pltpu.CompilerParams(
            vmem_limit_bytes=67043328, has_side_effects=True, collective_id=0
        ),
    )(
        queries,
        key_rows,
        value_rows,
        gates,
        gate_weight,
        up_weight,
        down_weight,
        out_weight,
        stream_in,
        mix_gain[None, :],
        mix_bias[None, :],
        ffn_gain[None, :],
        ffn_bias[None, :],
    )


def swap_cores(block):
    count = lax.axis_size("tp")
    return lax.ppermute(block, "tp", [(i, i ^ 1) for i in range(count)])


def swap_across(block):
    count = lax.axis_size("tp")
    return lax.ppermute(block, "tp", [(i, i ^ 2) for i in range(count)])


def body(
    queries,
    key_rows,
    value_rows,
    log_forget,
    stream_in,
    out_weight,
    mix_gain,
    mix_bias,
    gate_weight,
    up_weight,
    down_weight,
    ffn_gain,
    ffn_bias,
):
    length = queries.shape[0]
    heads = log_forget.shape[1]
    head_dim = queries.shape[1] // heads
    pieces, group = lax.axis_size("sp"), lax.axis_size("tp")
    by_head = heads == pieces and head_dim + 16 <= 128 and head_dim % 16 == 0
    if by_head and pieces == 8 and group == 4:
        return whole_layer(
            queries,
            key_rows,
            value_rows,
            log_forget,
            stream_in,
            out_weight,
            mix_gain,
            mix_bias,
            gate_weight,
            up_weight,
            down_weight,
            ffn_gain,
            ffn_bias,
        )
    gate_full = lax.all_gather(gate_weight, "sp", axis=0, tiled=True)
    up_full = lax.all_gather(up_weight, "sp", axis=0, tiled=True)
    down_full = lax.all_gather(down_weight, "sp", axis=1, tiled=True)
    turned = attend(queries, key_rows, value_rows, log_forget).T
    own_rows = length // lax.axis_size("tp")
    offset = lax.axis_index("tp") * own_rows
    two_level = lax.axis_size("tp") == 4
    partial_mix = lax.dot_general(
        turned, out_weight, (((0,), (0,)), ((), ())), preferred_element_type=jnp.float32
    ).astype(jnp.bfloat16)
    if two_level:
        core = lax.axis_index("tp") % 2
        across = lax.axis_index("tp") // 2
        split = partial_mix.reshape(2, 2, own_rows, -1)
        mine = lax.dynamic_index_in_dim(split, core, 1, keepdims=False)
        other = lax.dynamic_index_in_dim(split, 1 - core, 1, keepdims=False)
        both = mine.astype(jnp.float32) + swap_cores(other).astype(jnp.float32)
        own = lax.dynamic_index_in_dim(both, across, 0, keepdims=False)
        away = lax.dynamic_index_in_dim(both, 1 - across, 0, keepdims=False)
        summed = (own + swap_across(away.astype(jnp.bfloat16)).astype(jnp.float32)).astype(
            jnp.bfloat16
        )
    else:
        summed = lax.psum_scatter(partial_mix, "tp", scatter_dimension=0, tiled=True)
    mix_out = lax.optimization_barrier(summed).astype(jnp.float32)
    stream_own = lax.dynamic_slice_in_dim(stream_in, offset, own_rows, 0)
    normed = layer_norm(
        ALPHA * stream_own.astype(jnp.float32) + mix_out, mix_gain, mix_bias
    ).astype(jnp.bfloat16)
    if two_level:
        pair = jnp.concatenate([normed, swap_across(normed)], axis=0)
        gathered = jnp.concatenate([pair, swap_cores(pair)], axis=0)
    else:
        gathered = lax.all_gather(normed, "tp", axis=0, tiled=True)
    gate_part = jnp.dot(gathered, gate_full, preferred_element_type=jnp.float32)
    up_part = jnp.dot(gathered, up_full, preferred_element_type=jnp.float32)
    hidden = (jax.nn.silu(gate_part) * up_part).astype(jnp.bfloat16)
    if two_level:
        columns = []
        half = down_full.shape[1] // 2
        for start in (0, half):
            terms = jnp.dot(
                hidden, down_full[:, start : start + half], preferred_element_type=jnp.float32
            ).astype(jnp.bfloat16)
            both = terms[: 2 * own_rows].astype(jnp.float32) + swap_cores(
                terms[2 * own_rows :]
            ).astype(jnp.float32)
            columns.append(
                both[:own_rows]
                + swap_across(both[own_rows:].astype(jnp.bfloat16)).astype(jnp.float32)
            )
        lowered = jnp.concatenate(columns, axis=1)
    else:
        partial_terms = jnp.dot(hidden, down_full, preferred_element_type=jnp.float32)
        lowered = lax.psum_scatter(
            partial_terms.astype(jnp.bfloat16), "tp", scatter_dimension=0, tiled=True
        ).astype(jnp.float32)
    lowered = lax.optimization_barrier(lowered.astype(jnp.bfloat16)).astype(jnp.float32)
    result = layer_norm(ALPHA * normed.astype(jnp.float32) + lowered, ffn_gain, ffn_bias)
    return result.astype(jnp.bfloat16)


def solution(mesh):
    placed = (
        P("sp", "tp"),
        P("sp", "tp"),
        P("sp", "tp"),
        P("sp", "tp"),
        P("sp", None),
        P("tp", None),
        P(),
        P(),
        P("sp", "tp"),
        P("sp", "tp"),
        P("tp", "sp"),
        P(),
        P(),
    )
    return jax.shard_map(
        body, mesh=mesh, in_specs=placed, out_specs=P(("sp", "tp"), None), check_vma=False
    )
```

```python
import jax
import jax.numpy as jnp
from jax import lax
from jax.experimental import pallas as pl
from jax.experimental.pallas import tpu as pltpu
from jax.sharding import PartitionSpec as P


ALPHA = 8.0**0.25
EPSILON = 1e-05


def layer_norm(matrix, norm_gain, norm_shift):
    centred = matrix - jnp.mean(matrix, axis=-1, keepdims=True)
    spread = jnp.mean(centred * centred, axis=-1, keepdims=True)
    return centred * lax.rsqrt(spread + EPSILON) * norm_gain + norm_shift


def attend(queries, key_rows, value_rows, log_forget):
    length, row_width = queries.shape
    head_count = log_forget.shape[1]
    head_dim = row_width // head_count
    score_scale = head_dim ** (-0.5)
    first_pos = lax.axis_index("sp") * length
    last_pos = first_pos + length
    query_heads = queries.reshape(length, head_count, head_dim)
    query_gates = log_forget.T
    query_pos = first_pos + jnp.arange(length, dtype=jnp.int32)
    gates_all = lax.all_gather(log_forget, "sp", axis=0, tiled=True)
    initial = (
        jnp.full((head_count, length), -1e30, jnp.float32),
        jnp.zeros((head_count, length), jnp.float32),
        jnp.zeros((length, head_count, head_dim), jnp.float32),
    )
    running = initial
    key_piece = lax.all_gather(key_rows, "sp", axis=0, tiled=True)
    value_piece = lax.all_gather(value_rows, "sp", axis=0, tiled=True)
    piece_len = key_piece.shape[0]
    shards = piece_len // length
    group_size = max(
        [
            count_try
            for count_try in range(1, shards + 1)
            if shards % count_try == 0 and count_try * length <= max(length, 512)
        ]
    )
    block_len = group_size * length
    blocks = piece_len // block_len
    key_blocks = key_piece.reshape(blocks, block_len, head_count, head_dim)
    value_blocks = value_piece.reshape(blocks, block_len, head_count, head_dim)
    gate_blocks = gates_all.reshape(blocks, block_len, head_count)
    block_starts = block_len * jnp.arange(blocks, dtype=jnp.int32)

    def one_block(running_state, packed):
        key_block, value_block, gate_block, block_start = packed

        def compute(state_in):
            highest, totals, weighted = state_in
            scores = (
                jnp.einsum(
                    "qhd,khd->hqk", query_heads, key_block, preferred_element_type=jnp.float32
                )
                * score_scale
            )
            scores = scores + query_gates[:, :, None] - gate_block.T[:, None, :]
            key_pos = block_start + jnp.arange(block_len, dtype=jnp.int32)
            allowed = (key_pos[None, :] <= query_pos[:, None])[None]
            masked = jnp.where(allowed, scores, -1e30)
            new_high = jnp.maximum(highest, jnp.max(masked, axis=2))
            weights = jnp.where(allowed, jnp.exp(masked - new_high[:, :, None]), 0.0)
            factor = jnp.exp(highest - new_high)
            totals = totals * factor + jnp.sum(weights, axis=2)
            weighted = weighted * factor.T[:, :, None] + jnp.einsum(
                "hqk,khd->qhd",
                weights.astype(jnp.bfloat16),
                value_block,
                preferred_element_type=jnp.float32,
            )
            return (new_high, totals, weighted)

        def keep_state(state_in):
            return state_in

        return (lax.cond(block_start < last_pos, compute, keep_state, running_state), None)

    running, unused = lax.scan(
        one_block, running, (key_blocks, value_blocks, gate_blocks, block_starts)
    )
    highest, totals, weighted = running
    return (weighted / totals.T[:, :, None]).reshape(length, row_width).astype(jnp.bfloat16)


SUB = 256


def gate_pieces(log_forget):
    gates = log_forget.T
    high = lax.reduce_precision(gates, 8, 7)
    middle = lax.reduce_precision(gates - high, 8, 7)
    low = gates - high - middle
    rows = jnp.stack([high, middle, low], axis=1).astype(jnp.bfloat16)
    return jnp.pad(rows, ((0, 0), (0, 13), (0, 0)))


def flash_piece(index, recv, kk, vaug, qaug, high_ref, acc_ref, head_dim):
    length = recv.shape[2]
    sub = SUB if length % SUB == 0 else length
    scale = head_dim**-0.5
    gate_rows = recv.shape[1] - 3 * head_dim
    query_at = head_dim + gate_rows
    value_at = query_at + head_dim
    kk[index] = recv[index, 0:128, :].T
    vaug[index, 0:head_dim, :] = recv[index, value_at : value_at + head_dim, :]
    row_index = lax.broadcasted_iota(jnp.int32, (gate_rows, length), 0)
    vaug[index, head_dim : head_dim + gate_rows, :] = jnp.where(row_index < 1, 1.0, 0.0).astype(
        jnp.bfloat16
    )
    block = recv[index, query_at : query_at + head_dim, :]
    qaug[0:head_dim, :] = (block.astype(jnp.float32) * scale).astype(jnp.bfloat16)
    qaug[head_dim : head_dim + gate_rows, :] = jnp.where(row_index < 3, -1.0, 0.0).astype(
        jnp.bfloat16
    )
    qaug[head_dim + gate_rows : 128, :] = jnp.zeros(
        (128 - head_dim - gate_rows, length), jnp.bfloat16
    )
    high_ref[...] = jnp.full_like(high_ref, -1e30)
    acc_ref[...] = jnp.zeros_like(acc_ref)

    def pair(piece, diagonal):
        starts = range(0, length, sub)
        spans = [slice(start, start + sub) for start in starts]
        widths = [start + sub if diagonal else length for start in starts]
        all_scores = [
            jnp.dot(kk[piece, 0:width, :], qaug[:, span], preferred_element_type=jnp.float32)
            for span, width in zip(spans, widths)
        ]
        if diagonal:
            key_pos = lax.broadcasted_iota(jnp.int32, (sub, sub), 0)
            allowed = key_pos <= lax.broadcasted_iota(jnp.int32, (sub, sub), 1)
            cut = [jnp.where(allowed, scores[-sub:], -1e30) for scores in all_scores]
            all_scores = cut[:1] + [
                jnp.concatenate([scores[:-sub], last], axis=0)
                for scores, last in zip(all_scores[1:], cut[1:])
            ]
        for scores, span, width in zip(all_scores, spans, widths):
            old_high = high_ref[:, span]
            new_high = jnp.maximum(old_high, jnp.max(scores, axis=0, keepdims=True))
            weights = jnp.exp(scores - new_high).astype(jnp.bfloat16)
            factor = jnp.exp(old_high - new_high)
            high_ref[:, span] = new_high
            acc_ref[:, span] = acc_ref[:, span] * factor + jnp.dot(
                vaug[piece, :, 0:width], weights, preferred_element_type=jnp.float32
            )

    def earlier(piece, inner):
        pair(piece, False)
        return inner

    lax.fori_loop(0, index, earlier, 0)
    pair(index, True)
    return (acc_ref[0:head_dim, :] / acc_ref[head_dim : head_dim + 1, :]).astype(jnp.bfloat16)


def layer_kernel(
    q_ref,
    k_ref,
    v_ref,
    t_ref,
    g_ref,
    u_ref,
    d_ref,
    ow_ref,
    st_ref,
    mg_ref,
    mb_ref,
    fg_ref,
    fb_ref,
    out_ref,
    packed,
    recv,
    kk,
    vaug,
    qaug,
    high_ref,
    acc_ref,
    outp,
    att,
    attT,
    wt,
    wbuf,
    owv,
    stv,
    psend,
    precv,
    xs,
    xr,
    nb,
    hid,
    dsend,
    drecv,
    dacc,
    rsb,
    r1,
    local_sem,
    own_sem,
    a_send,
    a_recv,
    b_send,
    b_recv,
    y_send,
    y_recv,
    w_sem,
    z_send,
    z_recv,
    p_send,
    p_recv,
    x_send,
    x_recv,
    g_send,
    g_recv,
    d_send,
    d_recv,
    r_send,
    r_recv,
):
    n_sp = lax.axis_size("sp")
    sp = lax.axis_index("sp")
    tp = lax.axis_index("tp")
    z, y = sp // 2, sp % 2
    x, c = tp // 2, tp % 2
    slabs = n_sp // 2
    y_peer = (z * 2 + 1 - y, tp)
    x_peer = (sp, (1 - x) * 2 + c)
    c_peer = (sp, x * 2 + 1 - c)
    length = recv.shape[2]
    head_dim = outp.shape[1]
    rows = out_ref.shape[0]
    width = out_ref.shape[1]
    part = wt.shape[1] // 2
    cols = wt.shape[2]

    def remote(src, dst, send, receive, device):
        return pltpu.make_async_remote_copy(
            src_ref=src,
            dst_ref=dst,
            send_sem=send,
            recv_sem=receive,
            device_id=device,
            device_id_type=pl.DeviceIdType.MESH,
        )

    barrier = pltpu.get_barrier_semaphore()

    def greet(step, carry):
        pl.semaphore_signal(
            barrier,
            inc=1,
            device_id=((sp + step) % n_sp, tp),
            device_id_type=pl.DeviceIdType.MESH,
        )
        return carry

    lax.fori_loop(1, n_sp, greet, 0)
    for device in (x_peer, c_peer):
        pl.semaphore_signal(
            barrier, inc=1, device_id=device, device_id_type=pl.DeviceIdType.MESH
        )
    gate_rows = t_ref.shape[1]
    packed[:, head_dim : head_dim + gate_rows, :] = t_ref[...]
    for first, rows_ref in (
        (0, k_ref),
        (head_dim + gate_rows, q_ref),
        (2 * head_dim + gate_rows, v_ref),
    ):
        turned = rows_ref[...].T
        packed[:, first : first + head_dim, :] = turned.reshape(n_sp, head_dim, length)
    wt[0] = g_ref[...].T
    wt[1] = u_ref[...].T
    pl.semaphore_wait(barrier, n_sp + 1)

    def piece_copy(other):
        return remote(
            packed.at[other], recv.at[sp], a_send.at[other], a_recv.at[sp], (other, tp)
        )

    def piece_wait(source):
        remote(
            packed.at[source], recv.at[source], a_send.at[source], a_recv.at[source], (source, tp)
        ).wait_recv()

    own_piece = pltpu.make_async_copy(packed.at[sp], recv.at[sp], own_sem.at[0])
    own_piece.start()

    def send_piece(step, carry):
        piece_copy((sp + n_sp - step) % n_sp).start()
        return carry

    lax.fori_loop(1, n_sp, send_piece, 0)
    load_ow = pltpu.make_async_copy(ow_ref, owv, local_sem.at[0])
    load_st = pltpu.make_async_copy(st_ref.at[pl.ds(tp * rows, rows), :], stv, local_sem.at[1])
    load_ow.start()
    load_st.start()

    inner = (z > 0) & (z + 1 < slabs)

    def chunk(matrix, owner, count):
        return wbuf.at[matrix, :, pl.ds(pl.multiple_of(owner * cols, cols), count * cols)]

    def weight_rows(matrix, which):
        taken = pl.ds(which * part, part)
        return d_ref.at[taken, :] if matrix == 2 else wt.at[matrix, taken, :]

    def keep_copy(matrix):
        return pltpu.make_async_copy(
            weight_rows(matrix, y), chunk(matrix, sp, 1), w_sem.at[matrix]
        )

    def cross_copy(matrix):
        return remote(
            weight_rows(matrix, 1 - y),
            chunk(matrix, sp, 1),
            y_send.at[matrix],
            y_recv.at[matrix],
            y_peer,
        )

    def cross_wait(matrix):
        block = chunk(matrix, z * 2 + 1 - y, 1)
        remote(block, block, y_send.at[matrix], y_recv.at[matrix], y_peer).wait_recv()

    for matrix in range(2):
        cross_copy(matrix).start()
        keep_copy(matrix).start()
    keep_copy(2).start()

    def z_copy(way, stage, matrix, given, device):
        block = chunk(matrix, given * 2, 2)
        return remote(
            block,
            block,
            z_send.at[way, stage, matrix],
            z_recv.at[way, stage, matrix],
            (device, tp),
        )

    def z_start(way, stage, matrix, also=True):
        given = z - stage if way == 0 else z + stage
        allowed = (given >= 0) & (z + 1 < slabs) if way == 0 else (given < slabs) & (z >= 1)
        allowed = allowed & also

        @pl.when(allowed)
        def _():
            z_copy(way, stage, matrix, given, sp + 2 - 4 * way).start()

    def z_sent(way, stage, matrix):
        given = z - stage if way == 0 else z + stage
        allowed = (given >= 0) & (z + 1 < slabs) if way == 0 else (given < slabs) & (z >= 1)

        @pl.when(allowed)
        def _():
            z_copy(way, stage, matrix, given, sp + 2 - 4 * way).wait_send()

    def halves_ready(matrix):
        keep_copy(matrix).wait()
        part_start(matrix, y)

    def inward_start(matrix, also=True):
        for way in range(2):
            z_start(way, 0, matrix, (z // 2 == way) & also)

    def part_start(matrix, column):
        for way in range(2):
            device = sp + 2 - 4 * way

            @pl.when(inner & (z // 2 != way))
            def _():
                block = chunk(matrix, z * 2 + column, 1)
                remote(
                    block,
                    block,
                    z_send.at[way, 0, matrix],
                    z_recv.at[way, 0, matrix],
                    (device, tp),
                ).start()

    def weights_start():
        halves_ready(0)
        halves_ready(1)
        halves_ready(2)
        cross_wait(0)
        inward_start(0)
        part_start(0, 1 - y)
        cross_wait(1)
        inward_start(1, z != 1)
        part_start(1, 1 - y)

    def origin_of(order):
        upper = z // 2
        return (z, z + 1 - 2 * (z % 2), 2 - upper, 3 - 3 * upper)[order]

    def z_from(way):
        return sp - 2 + 4 * way

    def weights_arrive(matrix, order):
        origin = origin_of(order)
        for way in range(2):
            for stage in range(slabs - 1):

                @pl.when((z - origin if way == 0 else origin - z) == stage + 1)
                def _():
                    z_copy(way, stage, matrix, origin, z_from(way)).wait_recv()
                    if stage + 2 < slabs:
                        z_start(way, stage + 1, matrix)

    def relays(place):
        for at, slab, matrix, order in RELAYS:
            if at == place:

                @pl.when(inner if slab is None else z == slab)
                def _():
                    weights_arrive(matrix, order)

    def weights_end(matrix):
        @pl.when(jnp.logical_not(inner))
        def _():
            for order in range(1, slabs):
                weights_arrive(matrix, order)

    def back_copy(piece):
        return remote(
            outp.at[piece],
            att.at[pl.ds(sp * head_dim, head_dim), :],
            b_send.at[piece],
            b_recv.at[sp],
            (piece, tp),
        )

    def back_wait(source):
        remote(
            outp.at[source],
            att.at[pl.ds(source * head_dim, head_dim), :],
            b_send.at[source],
            b_recv.at[source],
            (source, tp),
        ).wait_recv()

    own_back = pltpu.make_async_copy(
        outp.at[sp], att.at[pl.ds(sp * head_dim, head_dim), :], own_sem.at[1]
    )

    def one_piece(index, carry):
        @pl.when(index == sp)
        def _():
            own_piece.wait()

        @pl.when(index != sp)
        def _():
            piece_wait(index)

        outp[index] = flash_piece(index, recv, kk, vaug, qaug, high_ref, acc_ref, head_dim)

        @pl.when(index == sp)
        def _():
            own_back.start()

        @pl.when(index != sp)
        def _():
            back_copy(index).start()

        @pl.when((index == START_AT) & (z == 0))
        def _():
            weights_start()

        @pl.when(index == CROSS_AT)
        def _():
            cross_copy(2).start()

        @pl.when(index == DOWN_AT)
        def _():
            cross_wait(2)
            part_start(2, 1 - y)

        for at in range(8):
            if any(relay[0] == at for relay in RELAYS):

                @pl.when(index == at)
                def _():
                    relays(at)

        return carry

    @pl.when(z > 0)
    def _():
        weights_start()

    lax.fori_loop(0, n_sp, one_piece, 0)
    inward_start(1, z == 1)
    relays("looped")
    inward_start(2)

    own_back.wait()

    def wait_back(step, carry):
        back_wait((sp + step) % n_sp)
        return carry

    lax.fori_loop(1, n_sp, wait_back, 0)
    load_ow.wait()
    load_st.wait()
    attT[...] = att[...].T

    def mix_block(owner):
        return jnp.dot(
            attT[pl.ds(owner * rows, rows), :], owv[...], preferred_element_type=jnp.float32
        )

    def pair_copy(slot):
        return remote(psend.at[slot], precv.at[slot], p_send.at[slot], p_recv.at[slot], c_peer)

    def mix_away(slot, carry):
        psend[slot] = mix_block(((x + 1 + slot) % 2) * 2 + 1 - c).astype(jnp.bfloat16)
        pair_copy(slot).start()
        return carry

    lax.fori_loop(0, 2, mix_away, 0)

    def mix_own(slot, carry):
        dacc[slot] = mix_block(((x + 1 + slot) % 2) * 2 + c)
        return carry

    lax.fori_loop(0, 2, mix_own, 0)
    pair_copy(0).wait_recv()
    xs[...] = (dacc[0] + precv[0].astype(jnp.float32)).astype(jnp.bfloat16)
    across = remote(xs, xr, x_send.at[0], x_recv.at[0], x_peer)
    across.start()
    relays("across")
    pair_copy(1).wait_recv()
    across.wait_recv()

    def place(by, bx, bc):
        return ((y + by) % 2) * 4 + ((x + bx) % 2) * 2 + (c + bc) % 2

    own = place(0, 0, 0)
    tile = 16

    def norm(matrix, gain, shift):
        centred = matrix - jnp.mean(matrix, axis=-1, keepdims=True)
        spread = jnp.mean(centred * centred, axis=-1, keepdims=True)
        return (centred * lax.rsqrt(spread + EPSILON) * gain + shift).astype(jnp.bfloat16)

    def mix_norm(step, carry):
        at = pl.ds(pl.multiple_of(step * tile, tile), tile)
        summed = dacc[1, at, :] + precv[1, at, :].astype(jnp.float32)
        summed = (summed + xr[at, :].astype(jnp.float32)).astype(jnp.bfloat16)
        nb[own, at, :] = norm(
            ALPHA * stv[at, :].astype(jnp.float32) + summed.astype(jnp.float32),
            mg_ref[...],
            mb_ref[...],
        )
        return carry

    lax.fori_loop(0, rows // tile, mix_norm, 0, unroll=2)

    top = pl.ds(0, rows // 2)
    bottom = pl.ds(rows // 2, rows // 2)

    def block_copy(sem, block, device):
        return remote(nb.at[block], nb.at[block], g_send.at[sem], g_recv.at[sem], device)

    def half_copy(sem, block, taken, device):
        view = nb.at[block, taken, :]
        return remote(view, view, g_send.at[sem], g_recv.at[sem], device)

    gathers = [
        block_copy(0, own, c_peer),
        block_copy(1, own, x_peer),
        block_copy(2, own, y_peer),
        half_copy(3, place(0, 1, 0), top, y_peer),
        half_copy(4, place(1, 0, 0), bottom, x_peer),
        block_copy(5, place(0, 1, 0), c_peer),
        block_copy(6, place(1, 0, 0), c_peer),
        block_copy(7, place(1, 1, 0), c_peer),
    ]
    arrivals = [
        block_copy(0, place(0, 0, 1), c_peer),
        block_copy(1, place(0, 1, 0), x_peer),
        block_copy(2, place(1, 0, 0), y_peer),
        half_copy(3, place(1, 1, 0), top, y_peer),
        half_copy(4, place(1, 1, 0), bottom, x_peer),
        block_copy(5, place(0, 1, 1), c_peer),
        block_copy(6, place(1, 0, 1), c_peer),
        block_copy(7, place(1, 1, 1), c_peer),
    ]
    gathers[1].start()
    gathers[2].start()
    gathers[0].start()
    relays("gather")

    def up_block(step):
        by, bx = step // 2, step % 2
        first = place(by, bx, 0) // 2
        block = nb[pl.ds(first * 2, 2)].reshape(2 * rows, width)
        contract = (((1,), (1,)), ((), ()))
        gate = lax.dot_general(block, wbuf[0], contract, preferred_element_type=jnp.float32)
        up = lax.dot_general(block, wbuf[1], contract, preferred_element_type=jnp.float32)
        hid[step] = (gate / (1.0 + jnp.exp(-gate)) * up).astype(jnp.bfloat16)

    arrivals[1].wait_recv()
    gathers[3].start()
    gathers[5].start()
    arrivals[2].wait_recv()
    gathers[4].start()
    gathers[6].start()
    arrivals[0].wait_recv()
    relays("gathered")
    weights_end(0)
    weights_end(1)

    def forward(step, carry):
        @pl.when(step == 1)
        def _():
            arrivals[5].wait_recv()

        @pl.when(step == 2)
        def _():
            arrivals[6].wait_recv()
            arrivals[3].wait_recv()
            arrivals[4].wait_recv()
            gathers[7].start()

        @pl.when(step == 3)
        def _():
            arrivals[7].wait_recv()

        up_block(step)
        return carry

    lax.fori_loop(0, 4, forward, 0)
    relays("upped")
    def span_of(origin, first, count):
        start = pl.multiple_of((origin * 2 + first) * cols, cols)
        return pl.ds(start, count * cols)

    def core_copy(step, origin):
        given = dsend.at[step, :, span_of(origin, 0, 2)]
        taken = drecv.at[step, :, span_of(origin, 0, 2)]
        return remote(given, taken, d_send.at[step, origin], d_recv.at[step, origin], c_peer)

    def out_copy(number, origin):
        slot, first, device = (
            (0, 0, x_peer),
            (1, 0, x_peer),
            (0, 1, y_peer),
            (2, 1, y_peer),
            (2, 0, y_peer),
            (1, 1, x_peer),
        )[number]
        return remote(
            rsb.at[slot, :, span_of(origin, first, 1)],
            r1.at[number, origin],
            r_send.at[number, origin],
            r_recv.at[number, origin],
            device,
        )

    def core_sum(step, origin):
        core_copy(step, origin).wait_recv()
        span = span_of(origin, 0, 2)
        summed = dacc[step, :, span] + drecv[step, :, span].astype(jnp.float32)
        dacc[step, :, span] = summed
        return summed.astype(jnp.bfloat16)

    def second_level(origin):
        out_copy(0, origin).wait_recv()
        near = span_of(origin, 0, 1)
        rsb[2, :, near] = (dacc[2, :, near] + r1[0, origin].astype(jnp.float32)).astype(
            jnp.bfloat16
        )
        out_copy(4, origin).start()
        out_copy(2, origin).wait_recv()
        near = span_of(origin, 1, 1)
        rsb[1, :, near] = (dacc[1, :, near] + r1[2, origin].astype(jnp.float32)).astype(
            jnp.bfloat16
        )
        out_copy(5, origin).start()

    def stage_origin(stage):
        upper = z // 2
        origin = jnp.where(stage == 1, z + 1 - 2 * (z % 2), 2 - upper)
        return jnp.where(stage == 0, z, jnp.where(stage == 3, 3 - 3 * upper, origin))

    def down_stage(stage, carry):
        origin = stage_origin(stage)

        @pl.when(stage == 3)
        def _():
            second_level(stage_origin(2))

        for order in range(1, slabs):

            @pl.when((stage == order) & jnp.logical_not(inner))
            def _():
                weights_arrive(2, order)

        span = span_of(origin, 0, 2)

        def down_step(step):
            slot = 3 - step
            slot = (slot // 2) + 2 * (slot % 2)
            given = hid[slot, pl.ds((1 - c) * rows, rows), :]
            dsend[step, :, span] = jnp.dot(
                given, wbuf[2, :, span], preferred_element_type=jnp.float32
            ).astype(jnp.bfloat16)
            core_copy(step, origin).start()
            kept = hid[slot, pl.ds(c * rows, rows), :]
            dacc[step, :, span] = jnp.dot(
                kept, wbuf[2, :, span], preferred_element_type=jnp.float32
            )

        down_step(0)
        down_step(1)
        rsb[0, :, span] = core_sum(0, origin)
        out_copy(0, origin).start()
        out_copy(2, origin).start()
        down_step(2)
        rsb[1, :, span_of(origin, 0, 1)] = core_sum(1, origin)[:, :cols]
        out_copy(1, origin).start()
        down_step(3)
        rsb[2, :, span_of(origin, 1, 1)] = core_sum(2, origin)[:, cols:]
        out_copy(3, origin).start()

        @pl.when((stage > 0) & (stage < 3))
        def _():
            second_level(stage_origin(stage - 1))

        core_sum(3, origin)
        return carry

    lax.fori_loop(0, 4, down_stage, 0)
    second_level(stage_origin(3))
    for number in (1, 3, 4, 5):
        for origin in range(4):
            out_copy(number, origin).wait_recv()

    def last_norm(step, carry):
        at = pl.ds(pl.multiple_of(step * tile, tile), tile)
        terms = []
        for origin in range(4):
            for first, one, two in ((0, 1, 4), (1, 3, 5)):
                start = (origin * 2 + first) * cols
                terms.append(
                    dacc[3, at, start : start + cols]
                    + r1[one, origin, at, :].astype(jnp.float32)
                    + r1[two, origin, at, :].astype(jnp.float32)
                )
        lowered = jnp.concatenate(terms, axis=1).astype(jnp.bfloat16).astype(jnp.float32)
        out_ref[at, :] = norm(
            ALPHA * nb[own, at, :].astype(jnp.float32) + lowered, fg_ref[...], fb_ref[...]
        )
        return carry

    lax.fori_loop(0, rows // tile, last_norm, 0, unroll=2)

    def sent_pieces(step, carry):
        piece_copy((sp + step) % n_sp).wait_send()
        back_copy((sp + step) % n_sp).wait_send()
        return carry

    lax.fori_loop(1, n_sp, sent_pieces, 0)
    for matrix in range(3):
        cross_copy(matrix).wait_send()
        for way in range(2):
            for stage in range(slabs - 1):
                z_sent(way, stage, matrix)

    pair_copy(0).wait_send()
    pair_copy(1).wait_send()
    across.wait_send()
    for copy in gathers:
        copy.wait_send()
    for origin in range(4):
        for step in range(4):
            core_copy(step, origin).wait_send()
        for number in range(6):
            out_copy(number, origin).wait_send()


START_AT = 2
CROSS_AT = 2
DOWN_AT = 6
RELAYS = (
    (5, 2, 0, 1),
    (5, 1, 0, 2),
    (7, None, 1, 2),
    ("looped", 1, 0, 1),
    (6, 2, 0, 2),
    ("looped", None, 1, 1),
    ("across", None, 0, 3),
    ("across", None, 2, 1),
    ("gather", None, 1, 3),
    ("gathered", None, 2, 2),
    ("upped", None, 2, 3),
)


def whole_layer(
    queries,
    key_rows,
    value_rows,
    log_forget,
    stream_in,
    out_weight,
    mix_gain,
    mix_bias,
    gate_weight,
    up_weight,
    down_weight,
    ffn_gain,
    ffn_bias,
):
    length, row_width = queries.shape
    heads = log_forget.shape[1]
    head_dim = row_width // heads
    pieces = lax.axis_size("sp")
    slabs = pieces // 2
    rows = length // lax.axis_size("tp")
    width = stream_in.shape[1]
    cols, hidden = gate_weight.shape
    part = hidden // 2
    gates = gate_pieces(log_forget)
    high_rows = head_dim + gates.shape[1]
    bf16, f32 = jnp.bfloat16, jnp.float32
    vmem, dma = pltpu.VMEM, pltpu.SemaphoreType.DMA
    scratch = [
        vmem((pieces, high_rows + 2 * head_dim, length), bf16),
        vmem((pieces, high_rows + 2 * head_dim, length), bf16),
        vmem((pieces, length, 128), bf16),
        vmem((pieces, high_rows, length), bf16),
        vmem((128, length), bf16),
        vmem((1, length), f32),
        vmem((high_rows, length), f32),
        vmem((pieces, head_dim, length), bf16),
        vmem((row_width, length), bf16),
        vmem((length, row_width), bf16),
        vmem((2, hidden, cols), bf16),
        vmem((3, part, width), bf16),
        vmem((row_width, width), bf16),
        vmem((rows, width), bf16),
        vmem((2, rows, width), bf16),
        vmem((2, rows, width), bf16),
        vmem((rows, width), bf16),
        vmem((rows, width), bf16),
        vmem((8, rows, width), bf16),
        vmem((4, 2 * rows, part), bf16),
        vmem((4, rows, width), bf16),
        vmem((4, rows, width), bf16),
        vmem((4, rows, width), f32),
        vmem((3, rows, width), bf16),
        vmem((6, 4, rows, cols), bf16),
        dma((2,)),
        dma((2,)),
        dma((pieces,)),
        dma((pieces,)),
        dma((pieces,)),
        dma((pieces,)),
        dma((3,)),
        dma((3,)),
        dma((3,)),
        dma((2, slabs - 1, 3)),
        dma((2, slabs - 1, 3)),
        dma((2,)),
        dma((2,)),
        dma((1,)),
        dma((1,)),
        dma((8,)),
        dma((8,)),
        dma((4, 4)),
        dma((4, 4)),
        dma((6, 4)),
        dma((6, 4)),
    ]
    in_vmem = pl.BlockSpec(memory_space=pltpu.VMEM)
    anywhere = pl.BlockSpec(memory_space=pl.ANY)
    return pl.pallas_call(
        layer_kernel,
        out_shape=jax.ShapeDtypeStruct((rows, width), bf16),
        in_specs=[in_vmem] * 6 + [anywhere] * 3 + [in_vmem] * 4,
        out_specs=in_vmem,
        scratch_shapes=scratch,
        compiler_params=pltpu.CompilerParams(
            vmem_limit_bytes=67043328, has_side_effects=True, collective_id=0
        ),
    )(
        queries,
        key_rows,
        value_rows,
        gates,
        gate_weight,
        up_weight,
        down_weight,
        out_weight,
        stream_in,
        mix_gain[None, :],
        mix_bias[None, :],
        ffn_gain[None, :],
        ffn_bias[None, :],
    )


def swap_cores(block):
    count = lax.axis_size("tp")
    return lax.ppermute(block, "tp", [(i, i ^ 1) for i in range(count)])


def swap_across(block):
    count = lax.axis_size("tp")
    return lax.ppermute(block, "tp", [(i, i ^ 2) for i in range(count)])


def body(
    queries,
    key_rows,
    value_rows,
    log_forget,
    stream_in,
    out_weight,
    mix_gain,
    mix_bias,
    gate_weight,
    up_weight,
    down_weight,
    ffn_gain,
    ffn_bias,
):
    length = queries.shape[0]
    heads = log_forget.shape[1]
    head_dim = queries.shape[1] // heads
    pieces, group = lax.axis_size("sp"), lax.axis_size("tp")
    by_head = heads == pieces and head_dim + 16 <= 128 and head_dim % 16 == 0
    if by_head and pieces == 8 and group == 4:
        return whole_layer(
            queries,
            key_rows,
            value_rows,
            log_forget,
            stream_in,
            out_weight,
            mix_gain,
            mix_bias,
            gate_weight,
            up_weight,
            down_weight,
            ffn_gain,
            ffn_bias,
        )
    gate_full = lax.all_gather(gate_weight, "sp", axis=0, tiled=True)
    up_full = lax.all_gather(up_weight, "sp", axis=0, tiled=True)
    down_full = lax.all_gather(down_weight, "sp", axis=1, tiled=True)
    turned = attend(queries, key_rows, value_rows, log_forget).T
    own_rows = length // lax.axis_size("tp")
    offset = lax.axis_index("tp") * own_rows
    two_level = lax.axis_size("tp") == 4
    partial_mix = lax.dot_general(
        turned, out_weight, (((0,), (0,)), ((), ())), preferred_element_type=jnp.float32
    ).astype(jnp.bfloat16)
    if two_level:
        core = lax.axis_index("tp") % 2
        across = lax.axis_index("tp") // 2
        split = partial_mix.reshape(2, 2, own_rows, -1)
        mine = lax.dynamic_index_in_dim(split, core, 1, keepdims=False)
        other = lax.dynamic_index_in_dim(split, 1 - core, 1, keepdims=False)
        both = mine.astype(jnp.float32) + swap_cores(other).astype(jnp.float32)
        own = lax.dynamic_index_in_dim(both, across, 0, keepdims=False)
        away = lax.dynamic_index_in_dim(both, 1 - across, 0, keepdims=False)
        summed = (own + swap_across(away.astype(jnp.bfloat16)).astype(jnp.float32)).astype(
            jnp.bfloat16
        )
    else:
        summed = lax.psum_scatter(partial_mix, "tp", scatter_dimension=0, tiled=True)
    mix_out = lax.optimization_barrier(summed).astype(jnp.float32)
    stream_own = lax.dynamic_slice_in_dim(stream_in, offset, own_rows, 0)
    normed = layer_norm(
        ALPHA * stream_own.astype(jnp.float32) + mix_out, mix_gain, mix_bias
    ).astype(jnp.bfloat16)
    if two_level:
        pair = jnp.concatenate([normed, swap_across(normed)], axis=0)
        gathered = jnp.concatenate([pair, swap_cores(pair)], axis=0)
    else:
        gathered = lax.all_gather(normed, "tp", axis=0, tiled=True)
    gate_part = jnp.dot(gathered, gate_full, preferred_element_type=jnp.float32)
    up_part = jnp.dot(gathered, up_full, preferred_element_type=jnp.float32)
    hidden = (jax.nn.silu(gate_part) * up_part).astype(jnp.bfloat16)
    if two_level:
        columns = []
        half = down_full.shape[1] // 2
        for start in (0, half):
            terms = jnp.dot(
                hidden, down_full[:, start : start + half], preferred_element_type=jnp.float32
            ).astype(jnp.bfloat16)
            both = terms[: 2 * own_rows].astype(jnp.float32) + swap_cores(
                terms[2 * own_rows :]
            ).astype(jnp.float32)
            columns.append(
                both[:own_rows]
                + swap_across(both[own_rows:].astype(jnp.bfloat16)).astype(jnp.float32)
            )
        lowered = jnp.concatenate(columns, axis=1)
    else:
        partial_terms = jnp.dot(hidden, down_full, preferred_element_type=jnp.float32)
        lowered = lax.psum_scatter(
            partial_terms.astype(jnp.bfloat16), "tp", scatter_dimension=0, tiled=True
        ).astype(jnp.float32)
    lowered = lax.optimization_barrier(lowered.astype(jnp.bfloat16)).astype(jnp.float32)
    result = layer_norm(ALPHA * normed.astype(jnp.float32) + lowered, ffn_gain, ffn_bias)
    return result.astype(jnp.bfloat16)


def solution(mesh):
    placed = (
        P("sp", "tp"),
        P("sp", "tp"),
        P("sp", "tp"),
        P("sp", "tp"),
        P("sp", None),
        P("tp", None),
        P(),
        P(),
        P("sp", "tp"),
        P("sp", "tp"),
        P("tp", "sp"),
        P(),
        P(),
    )
    return jax.shard_map(
        body, mesh=mesh, in_specs=placed, out_specs=P(("sp", "tp"), None), check_vma=False
    )
```

```python
import jax
import jax.numpy as jnp
from jax import lax
from jax.experimental import pallas as pl
from jax.experimental.pallas import tpu as pltpu
from jax.sharding import PartitionSpec as P


ALPHA = 8.0**0.25
EPSILON = 1e-05


def layer_norm(matrix, norm_gain, norm_shift):
    centred = matrix - jnp.mean(matrix, axis=-1, keepdims=True)
    spread = jnp.mean(centred * centred, axis=-1, keepdims=True)
    return centred * lax.rsqrt(spread + EPSILON) * norm_gain + norm_shift


def attend(queries, key_rows, value_rows, log_forget):
    length, row_width = queries.shape
    head_count = log_forget.shape[1]
    head_dim = row_width // head_count
    score_scale = head_dim ** (-0.5)
    first_pos = lax.axis_index("sp") * length
    last_pos = first_pos + length
    query_heads = queries.reshape(length, head_count, head_dim)
    query_gates = log_forget.T
    query_pos = first_pos + jnp.arange(length, dtype=jnp.int32)
    gates_all = lax.all_gather(log_forget, "sp", axis=0, tiled=True)
    initial = (
        jnp.full((head_count, length), -1e30, jnp.float32),
        jnp.zeros((head_count, length), jnp.float32),
        jnp.zeros((length, head_count, head_dim), jnp.float32),
    )
    running = initial
    key_piece = lax.all_gather(key_rows, "sp", axis=0, tiled=True)
    value_piece = lax.all_gather(value_rows, "sp", axis=0, tiled=True)
    piece_len = key_piece.shape[0]
    shards = piece_len // length
    group_size = max(
        [
            count_try
            for count_try in range(1, shards + 1)
            if shards % count_try == 0 and count_try * length <= max(length, 512)
        ]
    )
    block_len = group_size * length
    blocks = piece_len // block_len
    key_blocks = key_piece.reshape(blocks, block_len, head_count, head_dim)
    value_blocks = value_piece.reshape(blocks, block_len, head_count, head_dim)
    gate_blocks = gates_all.reshape(blocks, block_len, head_count)
    block_starts = block_len * jnp.arange(blocks, dtype=jnp.int32)

    def one_block(running_state, packed):
        key_block, value_block, gate_block, block_start = packed

        def compute(state_in):
            highest, totals, weighted = state_in
            scores = (
                jnp.einsum(
                    "qhd,khd->hqk", query_heads, key_block, preferred_element_type=jnp.float32
                )
                * score_scale
            )
            scores = scores + query_gates[:, :, None] - gate_block.T[:, None, :]
            key_pos = block_start + jnp.arange(block_len, dtype=jnp.int32)
            allowed = (key_pos[None, :] <= query_pos[:, None])[None]
            masked = jnp.where(allowed, scores, -1e30)
            new_high = jnp.maximum(highest, jnp.max(masked, axis=2))
            weights = jnp.where(allowed, jnp.exp(masked - new_high[:, :, None]), 0.0)
            factor = jnp.exp(highest - new_high)
            totals = totals * factor + jnp.sum(weights, axis=2)
            weighted = weighted * factor.T[:, :, None] + jnp.einsum(
                "hqk,khd->qhd",
                weights.astype(jnp.bfloat16),
                value_block,
                preferred_element_type=jnp.float32,
            )
            return (new_high, totals, weighted)

        def keep_state(state_in):
            return state_in

        return (lax.cond(block_start < last_pos, compute, keep_state, running_state), None)

    running, unused = lax.scan(
        one_block, running, (key_blocks, value_blocks, gate_blocks, block_starts)
    )
    highest, totals, weighted = running
    return (weighted / totals.T[:, :, None]).reshape(length, row_width).astype(jnp.bfloat16)


SUB = 256


def gate_pieces(log_forget):
    gates = log_forget.T
    high = lax.reduce_precision(gates, 8, 7)
    middle = lax.reduce_precision(gates - high, 8, 7)
    low = gates - high - middle
    rows = jnp.stack([high, middle, low], axis=1).astype(jnp.bfloat16)
    return jnp.pad(rows, ((0, 0), (0, 13), (0, 0)))


def flash_piece(index, recv, kk, vaug, qaug, high_ref, acc_ref, head_dim):
    length = recv.shape[2]
    sub = SUB if length % SUB == 0 else length
    scale = head_dim**-0.5
    gate_rows = recv.shape[1] - 3 * head_dim
    query_at = head_dim + gate_rows
    value_at = query_at + head_dim
    kk[index] = recv[index, 0:128, :].T
    vaug[index, 0:head_dim, :] = recv[index, value_at : value_at + head_dim, :]
    row_index = lax.broadcasted_iota(jnp.int32, (gate_rows, length), 0)
    vaug[index, head_dim : head_dim + gate_rows, :] = jnp.where(row_index < 1, 1.0, 0.0).astype(
        jnp.bfloat16
    )
    block = recv[index, query_at : query_at + head_dim, :]
    qaug[0:head_dim, :] = (block.astype(jnp.float32) * scale).astype(jnp.bfloat16)
    qaug[head_dim : head_dim + gate_rows, :] = jnp.where(row_index < 3, -1.0, 0.0).astype(
        jnp.bfloat16
    )
    qaug[head_dim + gate_rows : 128, :] = jnp.zeros(
        (128 - head_dim - gate_rows, length), jnp.bfloat16
    )
    high_ref[...] = jnp.full_like(high_ref, -1e30)
    acc_ref[...] = jnp.zeros_like(acc_ref)

    def pair(piece, diagonal):
        starts = range(0, length, sub)
        spans = [slice(start, start + sub) for start in starts]
        widths = [start + sub if diagonal else length for start in starts]
        all_scores = [
            jnp.dot(kk[piece, 0:width, :], qaug[:, span], preferred_element_type=jnp.float32)
            for span, width in zip(spans, widths)
        ]
        if diagonal:
            key_pos = lax.broadcasted_iota(jnp.int32, (sub, sub), 0)
            allowed = key_pos <= lax.broadcasted_iota(jnp.int32, (sub, sub), 1)
            cut = [jnp.where(allowed, scores[-sub:], -1e30) for scores in all_scores]
            all_scores = cut[:1] + [
                jnp.concatenate([scores[:-sub], last], axis=0)
                for scores, last in zip(all_scores[1:], cut[1:])
            ]
        for scores, span, width in zip(all_scores, spans, widths):
            old_high = high_ref[:, span]
            new_high = jnp.maximum(old_high, jnp.max(scores, axis=0, keepdims=True))
            weights = jnp.exp(scores - new_high).astype(jnp.bfloat16)
            factor = jnp.exp(old_high - new_high)
            high_ref[:, span] = new_high
            acc_ref[:, span] = acc_ref[:, span] * factor + jnp.dot(
                vaug[piece, :, 0:width], weights, preferred_element_type=jnp.float32
            )

    def earlier(piece, inner):
        pair(piece, False)
        return inner

    lax.fori_loop(0, index, earlier, 0)
    pair(index, True)
    return (acc_ref[0:head_dim, :] / acc_ref[head_dim : head_dim + 1, :]).astype(jnp.bfloat16)


def layer_kernel(
    q_ref,
    k_ref,
    v_ref,
    t_ref,
    g_ref,
    u_ref,
    d_ref,
    ow_ref,
    st_ref,
    mg_ref,
    mb_ref,
    fg_ref,
    fb_ref,
    out_ref,
    packed,
    recv,
    kk,
    vaug,
    qaug,
    high_ref,
    acc_ref,
    outp,
    att,
    attT,
    wt,
    wbuf,
    owv,
    stv,
    psend,
    precv,
    xs,
    xr,
    nb,
    hid,
    dsend,
    drecv,
    dacc,
    rsb,
    r1,
    local_sem,
    own_sem,
    a_send,
    a_recv,
    b_send,
    b_recv,
    y_send,
    y_recv,
    w_sem,
    z_send,
    z_recv,
    p_send,
    p_recv,
    x_send,
    x_recv,
    g_send,
    g_recv,
    d_send,
    d_recv,
    r_send,
    r_recv,
):
    n_sp = lax.axis_size("sp")
    sp = lax.axis_index("sp")
    tp = lax.axis_index("tp")
    z, y = sp // 2, sp % 2
    x, c = tp // 2, tp % 2
    slabs = n_sp // 2
    y_peer = (z * 2 + 1 - y, tp)
    x_peer = (sp, (1 - x) * 2 + c)
    c_peer = (sp, x * 2 + 1 - c)
    length = recv.shape[2]
    head_dim = outp.shape[1]
    rows = out_ref.shape[0]
    width = out_ref.shape[1]
    part = wt.shape[1] // 2
    cols = wt.shape[2]

    def remote(src, dst, send, receive, device):
        return pltpu.make_async_remote_copy(
            src_ref=src,
            dst_ref=dst,
            send_sem=send,
            recv_sem=receive,
            device_id=device,
            device_id_type=pl.DeviceIdType.MESH,
        )

    barrier = pltpu.get_barrier_semaphore()

    def greet(step, carry):
        pl.semaphore_signal(
            barrier,
            inc=1,
            device_id=((sp + step) % n_sp, tp),
            device_id_type=pl.DeviceIdType.MESH,
        )
        return carry

    lax.fori_loop(1, n_sp, greet, 0)
    for device in (x_peer, c_peer):
        pl.semaphore_signal(
            barrier, inc=1, device_id=device, device_id_type=pl.DeviceIdType.MESH
        )
    gate_rows = t_ref.shape[1]
    packed[:, head_dim : head_dim + gate_rows, :] = t_ref[...]
    for first, rows_ref in (
        (0, k_ref),
        (head_dim + gate_rows, q_ref),
        (2 * head_dim + gate_rows, v_ref),
    ):
        turned = rows_ref[...].T
        packed[:, first : first + head_dim, :] = turned.reshape(n_sp, head_dim, length)
    wt[0] = g_ref[...].T
    wt[1] = u_ref[...].T
    pl.semaphore_wait(barrier, n_sp + 1)

    def piece_copy(other):
        return remote(
            packed.at[other], recv.at[sp], a_send.at[other], a_recv.at[sp], (other, tp)
        )

    def piece_wait(source):
        remote(
            packed.at[source], recv.at[source], a_send.at[source], a_recv.at[source], (source, tp)
        ).wait_recv()

    own_piece = pltpu.make_async_copy(packed.at[sp], recv.at[sp], own_sem.at[0])
    own_piece.start()

    def send_piece(step, carry):
        piece_copy((sp + n_sp - step) % n_sp).start()
        return carry

    lax.fori_loop(1, n_sp, send_piece, 0)
    load_ow = pltpu.make_async_copy(ow_ref, owv, local_sem.at[0])
    load_st = pltpu.make_async_copy(st_ref.at[pl.ds(tp * rows, rows), :], stv, local_sem.at[1])
    load_ow.start()
    load_st.start()

    inner = (z > 0) & (z + 1 < slabs)

    def chunk(matrix, owner, count):
        return wbuf.at[matrix, :, pl.ds(pl.multiple_of(owner * cols, cols), count * cols)]

    def weight_rows(matrix, which):
        taken = pl.ds(which * part, part)
        return d_ref.at[taken, :] if matrix == 2 else wt.at[matrix, taken, :]

    def keep_copy(matrix):
        return pltpu.make_async_copy(
            weight_rows(matrix, y), chunk(matrix, sp, 1), w_sem.at[matrix]
        )

    def cross_copy(matrix):
        return remote(
            weight_rows(matrix, 1 - y),
            chunk(matrix, sp, 1),
            y_send.at[matrix],
            y_recv.at[matrix],
            y_peer,
        )

    def cross_wait(matrix):
        block = chunk(matrix, z * 2 + 1 - y, 1)
        remote(block, block, y_send.at[matrix], y_recv.at[matrix], y_peer).wait_recv()

    for matrix in range(2):
        cross_copy(matrix).start()
        keep_copy(matrix).start()
    keep_copy(2).start()

    def z_copy(way, stage, matrix, given, device):
        block = chunk(matrix, given * 2, 2)
        return remote(
            block,
            block,
            z_send.at[way, stage, matrix],
            z_recv.at[way, stage, matrix],
            (device, tp),
        )

    def z_start(way, stage, matrix, also=True):
        given = z - stage if way == 0 else z + stage
        allowed = (given >= 0) & (z + 1 < slabs) if way == 0 else (given < slabs) & (z >= 1)
        allowed = allowed & also

        @pl.when(allowed)
        def _():
            z_copy(way, stage, matrix, given, sp + 2 - 4 * way).start()

    def z_sent(way, stage, matrix):
        given = z - stage if way == 0 else z + stage
        allowed = (given >= 0) & (z + 1 < slabs) if way == 0 else (given < slabs) & (z >= 1)

        @pl.when(allowed)
        def _():
            z_copy(way, stage, matrix, given, sp + 2 - 4 * way).wait_send()

    def halves_ready(matrix):
        keep_copy(matrix).wait()
        part_start(matrix, y)

    def inward_start(matrix, also=True):
        for way in range(2):
            z_start(way, 0, matrix, (z // 2 == way) & also)

    def part_start(matrix, column):
        for way in range(2):
            device = sp + 2 - 4 * way

            @pl.when(inner & (z // 2 != way))
            def _():
                block = chunk(matrix, z * 2 + column, 1)
                remote(
                    block,
                    block,
                    z_send.at[way, 0, matrix],
                    z_recv.at[way, 0, matrix],
                    (device, tp),
                ).start()

    def weights_start():
        halves_ready(0)
        halves_ready(1)
        halves_ready(2)
        cross_wait(0)
        inward_start(0)
        part_start(0, 1 - y)
        cross_wait(1)
        inward_start(1, z != 1)
        part_start(1, 1 - y)

    def origin_of(order):
        upper = z // 2
        return (z, z + 1 - 2 * (z % 2), 2 - upper, 3 - 3 * upper)[order]

    def z_from(way):
        return sp - 2 + 4 * way

    def weights_arrive(matrix, order):
        origin = origin_of(order)
        for way in range(2):
            for stage in range(slabs - 1):

                @pl.when((z - origin if way == 0 else origin - z) == stage + 1)
                def _():
                    z_copy(way, stage, matrix, origin, z_from(way)).wait_recv()
                    if stage + 2 < slabs:
                        z_start(way, stage + 1, matrix)

    def relays(place):
        for at, slab, matrix, order in RELAYS:
            if at == place:

                @pl.when(inner if slab is None else z == slab)
                def _():
                    weights_arrive(matrix, order)

    def weights_end(matrix):
        @pl.when(jnp.logical_not(inner))
        def _():
            for order in range(1, slabs):
                weights_arrive(matrix, order)

    def back_copy(piece):
        return remote(
            outp.at[piece],
            att.at[pl.ds(sp * head_dim, head_dim), :],
            b_send.at[piece],
            b_recv.at[sp],
            (piece, tp),
        )

    def back_wait(source):
        remote(
            outp.at[source],
            att.at[pl.ds(source * head_dim, head_dim), :],
            b_send.at[source],
            b_recv.at[source],
            (source, tp),
        ).wait_recv()

    own_back = pltpu.make_async_copy(
        outp.at[sp], att.at[pl.ds(sp * head_dim, head_dim), :], own_sem.at[1]
    )

    def one_piece(index, carry):
        @pl.when(index == sp)
        def _():
            own_piece.wait()

        @pl.when(index != sp)
        def _():
            piece_wait(index)

        outp[index] = flash_piece(index, recv, kk, vaug, qaug, high_ref, acc_ref, head_dim)

        @pl.when(index == sp)
        def _():
            own_back.start()

        @pl.when(index != sp)
        def _():
            back_copy(index).start()

        @pl.when((index == START_AT) & (z == 0))
        def _():
            weights_start()

        @pl.when(index == CROSS_AT)
        def _():
            cross_copy(2).start()

        @pl.when(index == DOWN_AT)
        def _():
            cross_wait(2)
            part_start(2, 1 - y)

        for at in range(8):
            if any(relay[0] == at for relay in RELAYS):

                @pl.when(index == at)
                def _():
                    relays(at)

        return carry

    @pl.when(z > 0)
    def _():
        weights_start()

    lax.fori_loop(0, n_sp, one_piece, 0)
    inward_start(1, z == 1)
    relays("looped")
    inward_start(2)

    own_back.wait()

    def wait_back(step, carry):
        back_wait((sp + step) % n_sp)
        return carry

    lax.fori_loop(1, n_sp, wait_back, 0)
    load_ow.wait()
    load_st.wait()
    attT[...] = att[...].T

    def mix_block(owner):
        return jnp.dot(
            attT[pl.ds(owner * rows, rows), :], owv[...], preferred_element_type=jnp.float32
        )

    def pair_copy(slot):
        return remote(psend.at[slot], precv.at[slot], p_send.at[slot], p_recv.at[slot], c_peer)

    def mix_away(slot, carry):
        psend[slot] = mix_block(((x + 1 + slot) % 2) * 2 + 1 - c).astype(jnp.bfloat16)
        pair_copy(slot).start()
        return carry

    lax.fori_loop(0, 2, mix_away, 0)

    def mix_own(slot, carry):
        dacc[slot] = mix_block(((x + 1 + slot) % 2) * 2 + c)
        return carry

    lax.fori_loop(0, 2, mix_own, 0)
    pair_copy(0).wait_recv()
    xs[...] = (dacc[0] + precv[0].astype(jnp.float32)).astype(jnp.bfloat16)
    across = remote(xs, xr, x_send.at[0], x_recv.at[0], x_peer)
    across.start()
    relays("across")
    pair_copy(1).wait_recv()
    across.wait_recv()

    def place(by, bx, bc):
        return ((y + by) % 2) * 4 + ((x + bx) % 2) * 2 + (c + bc) % 2

    own = place(0, 0, 0)
    tile = 16

    def norm(matrix, gain, shift):
        centred = matrix - jnp.mean(matrix, axis=-1, keepdims=True)
        spread = jnp.mean(centred * centred, axis=-1, keepdims=True)
        return (centred * lax.rsqrt(spread + EPSILON) * gain + shift).astype(jnp.bfloat16)

    def mix_norm(step, carry):
        at = pl.ds(pl.multiple_of(step * tile, tile), tile)
        summed = dacc[1, at, :] + precv[1, at, :].astype(jnp.float32)
        summed = (summed + xr[at, :].astype(jnp.float32)).astype(jnp.bfloat16)
        nb[own, at, :] = norm(
            ALPHA * stv[at, :].astype(jnp.float32) + summed.astype(jnp.float32),
            mg_ref[...],
            mb_ref[...],
        )
        return carry

    lax.fori_loop(0, rows // tile, mix_norm, 0, unroll=4)

    top = pl.ds(0, rows // 2)
    bottom = pl.ds(rows // 2, rows // 2)

    def block_copy(sem, block, device):
        return remote(nb.at[block], nb.at[block], g_send.at[sem], g_recv.at[sem], device)

    def half_copy(sem, block, taken, device):
        view = nb.at[block, taken, :]
        return remote(view, view, g_send.at[sem], g_recv.at[sem], device)

    gathers = [
        block_copy(0, own, c_peer),
        block_copy(1, own, x_peer),
        block_copy(2, own, y_peer),
        half_copy(3, place(0, 1, 0), top, y_peer),
        half_copy(4, place(1, 0, 0), bottom, x_peer),
        block_copy(5, place(0, 1, 0), c_peer),
        block_copy(6, place(1, 0, 0), c_peer),
        block_copy(7, place(1, 1, 0), c_peer),
    ]
    arrivals = [
        block_copy(0, place(0, 0, 1), c_peer),
        block_copy(1, place(0, 1, 0), x_peer),
        block_copy(2, place(1, 0, 0), y_peer),
        half_copy(3, place(1, 1, 0), top, y_peer),
        half_copy(4, place(1, 1, 0), bottom, x_peer),
        block_copy(5, place(0, 1, 1), c_peer),
        block_copy(6, place(1, 0, 1), c_peer),
        block_copy(7, place(1, 1, 1), c_peer),
    ]
    gathers[1].start()
    gathers[2].start()
    gathers[0].start()
    relays("gather")

    def up_block(step):
        by, bx = step // 2, step % 2
        first = place(by, bx, 0) // 2
        block = nb[pl.ds(first * 2, 2)].reshape(2 * rows, width)
        contract = (((1,), (1,)), ((), ()))
        gate = lax.dot_general(block, wbuf[0], contract, preferred_element_type=jnp.float32)
        up = lax.dot_general(block, wbuf[1], contract, preferred_element_type=jnp.float32)
        hid[step] = (gate / (1.0 + jnp.exp(-gate)) * up).astype(jnp.bfloat16)

    arrivals[1].wait_recv()
    gathers[3].start()
    gathers[5].start()
    arrivals[2].wait_recv()
    gathers[4].start()
    gathers[6].start()
    arrivals[0].wait_recv()
    relays("gathered")
    weights_end(0)
    weights_end(1)

    def forward(step, carry):
        @pl.when(step == 1)
        def _():
            arrivals[5].wait_recv()

        @pl.when(step == 2)
        def _():
            arrivals[6].wait_recv()
            arrivals[3].wait_recv()
            arrivals[4].wait_recv()
            gathers[7].start()

        @pl.when(step == 3)
        def _():
            arrivals[7].wait_recv()

        up_block(step)
        return carry

    lax.fori_loop(0, 4, forward, 0)
    relays("upped")
    def span_of(origin, first, count):
        start = pl.multiple_of((origin * 2 + first) * cols, cols)
        return pl.ds(start, count * cols)

    def core_copy(step, origin):
        given = dsend.at[step, :, span_of(origin, 0, 2)]
        taken = drecv.at[step, :, span_of(origin, 0, 2)]
        return remote(given, taken, d_send.at[step, origin], d_recv.at[step, origin], c_peer)

    def out_copy(number, origin):
        slot, first, device = (
            (0, 0, x_peer),
            (1, 0, x_peer),
            (0, 1, y_peer),
            (2, 1, y_peer),
            (2, 0, y_peer),
            (1, 1, x_peer),
        )[number]
        return remote(
            rsb.at[slot, :, span_of(origin, first, 1)],
            r1.at[number, origin],
            r_send.at[number, origin],
            r_recv.at[number, origin],
            device,
        )

    def core_sum(step, origin):
        core_copy(step, origin).wait_recv()
        span = span_of(origin, 0, 2)
        summed = dacc[step, :, span] + drecv[step, :, span].astype(jnp.float32)
        dacc[step, :, span] = summed
        return summed.astype(jnp.bfloat16)

    def second_level(origin):
        out_copy(0, origin).wait_recv()
        near = span_of(origin, 0, 1)
        rsb[2, :, near] = (dacc[2, :, near] + r1[0, origin].astype(jnp.float32)).astype(
            jnp.bfloat16
        )
        out_copy(4, origin).start()
        out_copy(2, origin).wait_recv()
        near = span_of(origin, 1, 1)
        rsb[1, :, near] = (dacc[1, :, near] + r1[2, origin].astype(jnp.float32)).astype(
            jnp.bfloat16
        )
        out_copy(5, origin).start()

    def stage_origin(stage):
        upper = z // 2
        origin = jnp.where(stage == 1, z + 1 - 2 * (z % 2), 2 - upper)
        return jnp.where(stage == 0, z, jnp.where(stage == 3, 3 - 3 * upper, origin))

    def down_stage(stage, carry):
        origin = stage_origin(stage)

        @pl.when(stage == 3)
        def _():
            second_level(stage_origin(2))

        for order in range(1, slabs):

            @pl.when((stage == order) & jnp.logical_not(inner))
            def _():
                weights_arrive(2, order)

        span = span_of(origin, 0, 2)

        def down_step(step):
            slot = 3 - step
            slot = (slot // 2) + 2 * (slot % 2)
            given = hid[slot, pl.ds((1 - c) * rows, rows), :]
            dsend[step, :, span] = jnp.dot(
                given, wbuf[2, :, span], preferred_element_type=jnp.float32
            ).astype(jnp.bfloat16)
            core_copy(step, origin).start()
            kept = hid[slot, pl.ds(c * rows, rows), :]
            dacc[step, :, span] = jnp.dot(
                kept, wbuf[2, :, span], preferred_element_type=jnp.float32
            )

        down_step(0)
        down_step(1)
        rsb[0, :, span] = core_sum(0, origin)
        out_copy(0, origin).start()
        out_copy(2, origin).start()
        down_step(2)
        rsb[1, :, span_of(origin, 0, 1)] = core_sum(1, origin)[:, :cols]
        out_copy(1, origin).start()
        down_step(3)
        rsb[2, :, span_of(origin, 1, 1)] = core_sum(2, origin)[:, cols:]
        out_copy(3, origin).start()

        @pl.when((stage > 0) & (stage < 3))
        def _():
            second_level(stage_origin(stage - 1))

        core_sum(3, origin)
        return carry

    lax.fori_loop(0, 4, down_stage, 0)
    second_level(stage_origin(3))
    for number in (1, 3, 4, 5):
        for origin in range(4):
            out_copy(number, origin).wait_recv()

    def last_norm(step, carry):
        at = pl.ds(pl.multiple_of(step * tile, tile), tile)
        terms = []
        for origin in range(4):
            for first, one, two in ((0, 1, 4), (1, 3, 5)):
                start = (origin * 2 + first) * cols
                terms.append(
                    dacc[3, at, start : start + cols]
                    + r1[one, origin, at, :].astype(jnp.float32)
                    + r1[two, origin, at, :].astype(jnp.float32)
                )
        lowered = jnp.concatenate(terms, axis=1).astype(jnp.bfloat16).astype(jnp.float32)
        out_ref[at, :] = norm(
            ALPHA * nb[own, at, :].astype(jnp.float32) + lowered, fg_ref[...], fb_ref[...]
        )
        return carry

    lax.fori_loop(0, rows // tile, last_norm, 0, unroll=4)

    def sent_pieces(step, carry):
        piece_copy((sp + step) % n_sp).wait_send()
        back_copy((sp + step) % n_sp).wait_send()
        return carry

    lax.fori_loop(1, n_sp, sent_pieces, 0)
    for matrix in range(3):
        cross_copy(matrix).wait_send()
        for way in range(2):
            for stage in range(slabs - 1):
                z_sent(way, stage, matrix)

    pair_copy(0).wait_send()
    pair_copy(1).wait_send()
    across.wait_send()
    for copy in gathers:
        copy.wait_send()
    for origin in range(4):
        for step in range(4):
            core_copy(step, origin).wait_send()
        for number in range(6):
            out_copy(number, origin).wait_send()


START_AT = 2
CROSS_AT = 2
DOWN_AT = 6
RELAYS = (
    (5, 2, 0, 1),
    (5, 1, 0, 2),
    (7, None, 1, 2),
    ("looped", 1, 0, 1),
    (6, 2, 0, 2),
    ("looped", None, 1, 1),
    ("across", None, 0, 3),
    ("across", None, 2, 1),
    ("gather", None, 1, 3),
    ("gathered", None, 2, 2),
    ("upped", None, 2, 3),
)


def whole_layer(
    queries,
    key_rows,
    value_rows,
    log_forget,
    stream_in,
    out_weight,
    mix_gain,
    mix_bias,
    gate_weight,
    up_weight,
    down_weight,
    ffn_gain,
    ffn_bias,
):
    length, row_width = queries.shape
    heads = log_forget.shape[1]
    head_dim = row_width // heads
    pieces = lax.axis_size("sp")
    slabs = pieces // 2
    rows = length // lax.axis_size("tp")
    width = stream_in.shape[1]
    cols, hidden = gate_weight.shape
    part = hidden // 2
    gates = gate_pieces(log_forget)
    high_rows = head_dim + gates.shape[1]
    bf16, f32 = jnp.bfloat16, jnp.float32
    vmem, dma = pltpu.VMEM, pltpu.SemaphoreType.DMA
    scratch = [
        vmem((pieces, high_rows + 2 * head_dim, length), bf16),
        vmem((pieces, high_rows + 2 * head_dim, length), bf16),
        vmem((pieces, length, 128), bf16),
        vmem((pieces, high_rows, length), bf16),
        vmem((128, length), bf16),
        vmem((1, length), f32),
        vmem((high_rows, length), f32),
        vmem((pieces, head_dim, length), bf16),
        vmem((row_width, length), bf16),
        vmem((length, row_width), bf16),
        vmem((2, hidden, cols), bf16),
        vmem((3, part, width), bf16),
        vmem((row_width, width), bf16),
        vmem((rows, width), bf16),
        vmem((2, rows, width), bf16),
        vmem((2, rows, width), bf16),
        vmem((rows, width), bf16),
        vmem((rows, width), bf16),
        vmem((8, rows, width), bf16),
        vmem((4, 2 * rows, part), bf16),
        vmem((4, rows, width), bf16),
        vmem((4, rows, width), bf16),
        vmem((4, rows, width), f32),
        vmem((3, rows, width), bf16),
        vmem((6, 4, rows, cols), bf16),
        dma((2,)),
        dma((2,)),
        dma((pieces,)),
        dma((pieces,)),
        dma((pieces,)),
        dma((pieces,)),
        dma((3,)),
        dma((3,)),
        dma((3,)),
        dma((2, slabs - 1, 3)),
        dma((2, slabs - 1, 3)),
        dma((2,)),
        dma((2,)),
        dma((1,)),
        dma((1,)),
        dma((8,)),
        dma((8,)),
        dma((4, 4)),
        dma((4, 4)),
        dma((6, 4)),
        dma((6, 4)),
    ]
    in_vmem = pl.BlockSpec(memory_space=pltpu.VMEM)
    anywhere = pl.BlockSpec(memory_space=pl.ANY)
    return pl.pallas_call(
        layer_kernel,
        out_shape=jax.ShapeDtypeStruct((rows, width), bf16),
        in_specs=[in_vmem] * 6 + [anywhere] * 3 + [in_vmem] * 4,
        out_specs=in_vmem,
        scratch_shapes=scratch,
        compiler_params=pltpu.CompilerParams(
            vmem_limit_bytes=67043328, has_side_effects=True, collective_id=0
        ),
    )(
        queries,
        key_rows,
        value_rows,
        gates,
        gate_weight,
        up_weight,
        down_weight,
        out_weight,
        stream_in,
        mix_gain[None, :],
        mix_bias[None, :],
        ffn_gain[None, :],
        ffn_bias[None, :],
    )


def swap_cores(block):
    count = lax.axis_size("tp")
    return lax.ppermute(block, "tp", [(i, i ^ 1) for i in range(count)])


def swap_across(block):
    count = lax.axis_size("tp")
    return lax.ppermute(block, "tp", [(i, i ^ 2) for i in range(count)])


def body(
    queries,
    key_rows,
    value_rows,
    log_forget,
    stream_in,
    out_weight,
    mix_gain,
    mix_bias,
    gate_weight,
    up_weight,
    down_weight,
    ffn_gain,
    ffn_bias,
):
    length = queries.shape[0]
    heads = log_forget.shape[1]
    head_dim = queries.shape[1] // heads
    pieces, group = lax.axis_size("sp"), lax.axis_size("tp")
    by_head = heads == pieces and head_dim + 16 <= 128 and head_dim % 16 == 0
    if by_head and pieces == 8 and group == 4:
        return whole_layer(
            queries,
            key_rows,
            value_rows,
            log_forget,
            stream_in,
            out_weight,
            mix_gain,
            mix_bias,
            gate_weight,
            up_weight,
            down_weight,
            ffn_gain,
            ffn_bias,
        )
    gate_full = lax.all_gather(gate_weight, "sp", axis=0, tiled=True)
    up_full = lax.all_gather(up_weight, "sp", axis=0, tiled=True)
    down_full = lax.all_gather(down_weight, "sp", axis=1, tiled=True)
    turned = attend(queries, key_rows, value_rows, log_forget).T
    own_rows = length // lax.axis_size("tp")
    offset = lax.axis_index("tp") * own_rows
    two_level = lax.axis_size("tp") == 4
    partial_mix = lax.dot_general(
        turned, out_weight, (((0,), (0,)), ((), ())), preferred_element_type=jnp.float32
    ).astype(jnp.bfloat16)
    if two_level:
        core = lax.axis_index("tp") % 2
        across = lax.axis_index("tp") // 2
        split = partial_mix.reshape(2, 2, own_rows, -1)
        mine = lax.dynamic_index_in_dim(split, core, 1, keepdims=False)
        other = lax.dynamic_index_in_dim(split, 1 - core, 1, keepdims=False)
        both = mine.astype(jnp.float32) + swap_cores(other).astype(jnp.float32)
        own = lax.dynamic_index_in_dim(both, across, 0, keepdims=False)
        away = lax.dynamic_index_in_dim(both, 1 - across, 0, keepdims=False)
        summed = (own + swap_across(away.astype(jnp.bfloat16)).astype(jnp.float32)).astype(
            jnp.bfloat16
        )
    else:
        summed = lax.psum_scatter(partial_mix, "tp", scatter_dimension=0, tiled=True)
    mix_out = lax.optimization_barrier(summed).astype(jnp.float32)
    stream_own = lax.dynamic_slice_in_dim(stream_in, offset, own_rows, 0)
    normed = layer_norm(
        ALPHA * stream_own.astype(jnp.float32) + mix_out, mix_gain, mix_bias
    ).astype(jnp.bfloat16)
    if two_level:
        pair = jnp.concatenate([normed, swap_across(normed)], axis=0)
        gathered = jnp.concatenate([pair, swap_cores(pair)], axis=0)
    else:
        gathered = lax.all_gather(normed, "tp", axis=0, tiled=True)
    gate_part = jnp.dot(gathered, gate_full, preferred_element_type=jnp.float32)
    up_part = jnp.dot(gathered, up_full, preferred_element_type=jnp.float32)
    hidden = (jax.nn.silu(gate_part) * up_part).astype(jnp.bfloat16)
    if two_level:
        columns = []
        half = down_full.shape[1] // 2
        for start in (0, half):
            terms = jnp.dot(
                hidden, down_full[:, start : start + half], preferred_element_type=jnp.float32
            ).astype(jnp.bfloat16)
            both = terms[: 2 * own_rows].astype(jnp.float32) + swap_cores(
                terms[2 * own_rows :]
            ).astype(jnp.float32)
            columns.append(
                both[:own_rows]
                + swap_across(both[own_rows:].astype(jnp.bfloat16)).astype(jnp.float32)
            )
        lowered = jnp.concatenate(columns, axis=1)
    else:
        partial_terms = jnp.dot(hidden, down_full, preferred_element_type=jnp.float32)
        lowered = lax.psum_scatter(
            partial_terms.astype(jnp.bfloat16), "tp", scatter_dimension=0, tiled=True
        ).astype(jnp.float32)
    lowered = lax.optimization_barrier(lowered.astype(jnp.bfloat16)).astype(jnp.float32)
    result = layer_norm(ALPHA * normed.astype(jnp.float32) + lowered, ffn_gain, ffn_bias)
    return result.astype(jnp.bfloat16)


def solution(mesh):
    placed = (
        P("sp", "tp"),
        P("sp", "tp"),
        P("sp", "tp"),
        P("sp", "tp"),
        P("sp", None),
        P("tp", None),
        P(),
        P(),
        P("sp", "tp"),
        P("sp", "tp"),
        P("tp", "sp"),
        P(),
        P(),
    )
    return jax.shard_map(
        body, mesh=mesh, in_specs=placed, out_specs=P(("sp", "tp"), None), check_vma=False
    )
```
